32 devices in a mesh: ep: 8 (over z, x), tp: 4 (over y, core).
Axes of the slice: x: 2, y: 2, z: 4, core: 2. Of those that a mesh axis runs over, the one named last changes fastest.
Arguments:
- queries: bfloat16 [4096, 2048], P('ep', 'tp'), may hold values from -6 to 6
- keys: bfloat16 [4096, 2048], P('ep', 'tp'), may hold values from -12 to 12
- values: bfloat16 [4096, 2048], P('ep', 'tp'), may hold values from -8 to 8
- key_bias: bfloat16 [4096, 16], P('ep', 'tp'), may hold values from -16 to 0
- out_weight: bfloat16 [2048, 2048], P('tp'), may hold values from -0.1875 to 0.1875
- moe_input: bfloat16 [1024, 2048], P('ep'), may hold values from -6 to 6
- moe_gain: float32 [2048], replicated, may hold values from 0.1 to 1.9
- route_ids: int32 [1024, 2], P('ep'), may hold values from 0 to 7, all different within a row; in each aligned block of 128 rows (0 to 127, 128 to 255, ...) at most 48 rows name the same one
- route_scores: float32 [1024, 2], P('ep'), may hold values from 0.05 to 1
- shared_gate: bfloat16 [2048, 2048], P(None, 'tp'), may hold values from -0.125 to 0.125
- shared_up: bfloat16 [2048, 2048], P(None, 'tp'), may hold values from -0.125 to 0.125
- shared_down: bfloat16 [2048, 2048], P('tp'), may hold values from -0.1875 to 0.1875
- expert_gate: bfloat16 [8, 2048, 2048], P('ep', None, 'tp'), may hold values from -0.125 to 0.125
- expert_up: bfloat16 [8, 2048, 2048], P('ep', None, 'tp'), may hold values from -0.125 to 0.125
- expert_down: bfloat16 [8, 2048, 2048], P('ep', 'tp'), may hold values from -0.1875 to 0.1875
Outputs:
- mixed_tokens: bfloat16 [4096, 2048], P('ep', 'tp')
- expert_mix: bfloat16 [1024, 2048], P('ep', 'tp')
The draws below stay inside these ranges and needn't reach their ends.
Inputs may be any that keep to these rules, and one draw needn't show every extreme that they name: `route_ids`: each row names 2 different experts. Among the 128 rows of one index of ep no expert is named by more than 48 rows, and in some such block one expert is named by exactly 48 rows.
All inputs are finite; a program needn't handle non-finite values.
Results may differ from the reference program's by a relative error of at most 0.019.
Values may be sent and summed in bfloat16 or wider, within the bound.
A program may use at most 128 MiB of HBM per device.

```python
import math
import jax
import jax.numpy as jnp
import numpy as np
from jax import lax

D = 2048
HEADS = 16
HD = 128
F = 2048
FSH = 2048
TOPK = 2
SEQUENCE_COUNT = 1
ROWS_A = 512
ROWS_M = 128
ATTENTION_TOKENS = 4096
SEQUENCE_LENGTH = 4096
TOKENS_M = 1024
EXPERTS = 8
CAP = 48
N_EP = 8
N_TP = 4


def draw_key_bias(key, part):
    draw_keys = jax.random.split(key, 7)
    fast_share = 0.5
    fast_head = jax.random.uniform(draw_keys[0], (HEADS,)) < fast_share
    fast_rate = jnp.exp(jax.random.uniform(draw_keys[1], (HEADS,), minval=jnp.log(1.0 / 100.0), maxval=jnp.log(1.0 / 30.0)))
    slow_rate = jnp.exp(jax.random.uniform(draw_keys[2], (HEADS,), minval=jnp.log(0.3 / SEQUENCE_LENGTH), maxval=jnp.log(1.2 / SEQUENCE_LENGTH)))
    base_logit = jnp.log(jnp.where(fast_head, fast_rate, slow_rate)) - 2.15
    block_count = ATTENTION_TOKENS // ROWS_A
    block_shift = jax.random.uniform(draw_keys[3], (block_count, 1, HEADS), minval=-0.7, maxval=0.7)
    jitter = jax.random.uniform(draw_keys[4], (block_count, ROWS_A, HEADS), minval=-0.7, maxval=0.7)
    smoothing_factor = (base_logit[None, None, :] + block_shift + jitter).reshape(ATTENTION_TOKENS, HEADS)
    spike_position = jax.random.randint(draw_keys[5], (SEQUENCE_COUNT, 2), 0, SEQUENCE_LENGTH)
    token_position = jnp.arange(ATTENTION_TOKENS) % SEQUENCE_LENGTH
    sequence_index = jnp.arange(ATTENTION_TOKENS) // SEQUENCE_LENGTH
    spike_mask = jnp.any(token_position[:, None] == spike_position[sequence_index], axis=1)
    spike_fraction = jax.random.uniform(draw_keys[6], (ATTENTION_TOKENS, 1), minval=0.2, maxval=0.4)
    spike_logit = jnp.log(spike_fraction) - jnp.log(1.0 - spike_fraction)
    return jnp.where(spike_mask[:, None], spike_logit, smoothing_factor).astype(jnp.float32).astype(jnp.bfloat16)


def draw_values(key, part):
    draw_keys = jax.random.split(key, 3)
    block_count = ATTENTION_TOKENS // ROWS_A
    sign = jnp.where(jax.random.uniform(draw_keys[0], (HEADS,)) < 0.5, -1.0, 1.0)
    size = jax.random.uniform(draw_keys[1], (block_count, 1, HEADS, 1), minval=0.5, maxval=1.5)
    noise = jnp.clip(1.5 * jax.random.normal(draw_keys[2], (block_count, ROWS_A, HEADS, HD)), -6.0, 6.0)
    mixed = sign[None, None, :, None] * size + noise
    return mixed.reshape(ATTENTION_TOKENS, HEADS * HD).astype(jnp.float32).astype(jnp.bfloat16)


def with_spikes(array, rng, source, target, blocks, factor):
    def block_of(axis_at):
        return (jnp.arange(array.shape[axis_at]) // (array.shape[axis_at] // blocks)).reshape((-1,) + (1,) * (array.ndim - 1 - axis_at))

    one_side = jax.random.permutation(rng, blocks)[block_of(target)]
    far = (block_of(target) + blocks // 2) % blocks
    return jnp.where((block_of(source) == one_side) | (block_of(source) == far), factor * array, array)


def level_of(rng, extent, cuts, low, top_value):
    gain = 1.0
    for position, shards_of in cuts:
        heights = jax.random.uniform(jax.random.fold_in(jax.random.fold_in(rng, 6), position), (shards_of,), jnp.float32, low / len(cuts), top_value / len(cuts))
        gain = gain * jnp.repeat(jnp.exp(heights), extent[position] // shards_of).reshape((-1,) + (1,) * (len(extent) - 1 - position))
    return gain


def routed_block(key, own, number, rows, count, top, most, slope):
    order = jax.random.permutation(key, count)
    crowded, usual = portions_of(count, rows * top, most, slope, True), portions_of(count, rows * top, most, slope, False)
    places = jnp.arange(count)

    def named(lengths, offset_by):
        used = int((lengths > 0).sum())
        fixed = max(1, used // 4)
        shifted = fixed + (places - fixed + offset_by * (used - fixed)) % max(1, count - fixed)
        return jnp.zeros((count,), jnp.int32).at[order[jnp.where(places < fixed, places, shifted)]].set(jnp.asarray(lengths, jnp.int32))

    lengths = jnp.where(number % 4 == 0, named(crowded, number // 4), named(usual, number - number // 4 - 1))
    mixed = jax.random.permutation(jax.random.fold_in(own, 3), count)
    donor, sink = mixed[0:count // 2 * 2:2], mixed[1:count // 2 * 2:2]
    slack = jnp.minimum(lengths[donor] - 1, most - lengths[sink]) // 2
    slack = jnp.where((donor == order[0]) | (sink == order[0]) | (lengths[sink] == 0), 0, jnp.maximum(slack, 0))
    shifted = jax.random.randint(jax.random.fold_in(own, 4), (count // 2,), 0, 1 << 20) % (slack + 1)
    lengths = lengths.at[donor].add(-shifted).at[sink].add(shifted)
    members = jnp.searchsorted(jnp.cumsum(lengths), jnp.arange(rows * top), side="right").astype(jnp.int32)
    table = members.reshape(top, rows).T
    table = table[jax.random.permutation(jax.random.fold_in(own, 1), rows)]
    offset_by = jax.random.randint(jax.random.fold_in(own, 2), (rows, 1), 0, top)
    return jnp.take_along_axis(table, (jnp.arange(top)[None, :] + offset_by) % top, axis=1)


def portions_of(count, total, limit, lean, full):
    portions = [(1 << 20) // math.isqrt(standing ** lean) + 1 for standing in range(1, count + 1)]
    largest = limit if full else min(limit, max(-(-total // count), total * portions[0] // sum(portions)))
    least = 1 if total - largest >= count - 1 else 0
    holding, surplus = [largest] + [least] * (count - 1), total - largest - least * (count - 1)
    while surplus > 0:
        free = [i for i in range(1, count) if holding[i] < largest] or [i for i in range(1, count) if holding[i] < limit]
        mass, left = sum([portions[i] for i in free]), surplus
        for i in free:
            extra = min(limit - holding[i], max(1, left * portions[i] // mass), surplus)
            holding[i] = holding[i] + extra
            surplus = surplus - extra
    return np.array(holding)


def centred(rng, extent, deviation, most, shards=(), kind=jnp.bfloat16):
    gain = level_of(rng, extent, shards, -0.22, 0.18) if shards else 1.0
    values = jax.random.normal(rng, extent, jnp.float32) * deviation * gain
    return jnp.minimum(jnp.maximum(values, -most), most).astype(kind)


def gaussian_with(stream_key, dims, scale, limit, shards, heavy, held_as=jnp.bfloat16):
    array = scale * jax.random.normal(stream_key, dims, jnp.float32)
    if shards:
        array = array * level_of(stream_key, dims, shards, -0.22, 0.18)
    return jnp.clip(with_spikes(array, jax.random.fold_in(stream_key, 3), *heavy), -limit, limit).astype(held_as)


def setup_inputs(seed: int = 0) -> dict:
    streams_of = jax.random.split(jax.random.key(seed), 16)
    queries = centred(streams_of[0], (ATTENTION_TOKENS, HEADS * HD), 1.0, 6.0, ((0, 8), (1, 4)))
    keys = centred(streams_of[1], (ATTENTION_TOKENS, HEADS * HD), 2.0, 12.0, ((0, 8), (1, 4)))
    values = draw_values(jax.random.fold_in(streams_of[15], 71), 0)
    key_bias = draw_key_bias(jax.random.fold_in(streams_of[15], 71), 0)
    out_weight = gaussian_with(streams_of[4], (HEADS * HD, D), (HEADS * HD) ** -0.5, 0.1875, ((0, 4),), (0, 1, 4, 2.0))
    moe_input = centred(streams_of[5], (TOKENS_M, D), 1.0, 6.0, ((0, 8),))
    moe_gain = jnp.clip(1.0 + 0.18 * jax.random.normal(streams_of[6], (D,), jnp.float32), 0.1, 1.9)
    route_ids_keys = jax.random.split(jax.random.fold_in(streams_of[7], 1), TOKENS_M // ROWS_M)
    route_ids_turns = jax.random.permutation(jax.random.fold_in(streams_of[7], 3), TOKENS_M // ROWS_M)
    route_ids = jax.vmap(lambda own, number: routed_block(jax.random.fold_in(streams_of[7], 2), own, number, ROWS_M, EXPERTS, TOPK, CAP, 2))(route_ids_keys, route_ids_turns).reshape((TOKENS_M, TOPK))
    route_scores = jnp.clip(0.05 + 0.95 * jax.random.uniform(streams_of[8], (TOKENS_M, TOPK), jnp.float32) ** level_of(streams_of[8], (TOKENS_M, TOPK), ((0, 8),), -0.2, 0.2), 0.05, 1.0)
    shared_gate = centred(streams_of[9], (D, FSH), D ** -0.5, 0.125, ((1, 4),))
    shared_up = centred(streams_of[10], (D, FSH), D ** -0.5, 0.125, ((1, 4),))
    shared_down = gaussian_with(streams_of[11], (FSH, D), FSH ** -0.5, 0.1875, ((0, 4),), (0, 1, 4, 2.0))
    expert_gate = centred(streams_of[12], (EXPERTS, D, F), D ** -0.5, 0.125, ((0, 8), (2, 4)))
    expert_up = centred(streams_of[13], (EXPERTS, D, F), D ** -0.5, 0.125, ((0, 8), (2, 4)))
    expert_down = gaussian_with(streams_of[14], (EXPERTS, F, D), F ** -0.5, 0.1875, ((0, 8), (1, 4)), (1, 2, 4, 2.0))
    return {"queries": queries, "keys": keys, "values": values, "key_bias": key_bias, "out_weight": out_weight, "moe_input": moe_input, "moe_gain": moe_gain, "route_ids": route_ids, "route_scores": route_scores, "shared_gate": shared_gate, "shared_up": shared_up, "shared_down": shared_down, "expert_gate": expert_gate, "expert_up": expert_up, "expert_down": expert_down}


EPS_NORM = 1e-06
ROUTED_SCALE = 2.5

def head_span(query_head, key_head, value_head, bias_head):
    length = query_head.shape[0]
    block = min(512, length)
    scale = HD ** (-0.5)
    key_pos = jnp.arange(length, dtype=jnp.int32)
    bias_row = bias_head.astype(jnp.float32)[None, :]

    def one_block(start):
        query_block = lax.dynamic_slice_in_dim(query_head, start, block, 0)
        logit = jnp.dot(query_block, key_head.T, preferred_element_type=jnp.float32) * scale + bias_row
        query_pos = start + jnp.arange(block, dtype=jnp.int32)
        visible = key_pos[None, :] < query_pos[:, None]
        keep = jnp.where(visible, jax.nn.log_sigmoid(-logit), 0.0)
        stay = lax.cumsum(keep, axis=1, reverse=True) - keep
        weight = jnp.where(visible, jnp.exp(jax.nn.log_sigmoid(logit) + stay), 0.0).astype(jnp.bfloat16)
        return jnp.dot(weight, value_head, preferred_element_type=jnp.float32).astype(jnp.bfloat16)
    starts = jnp.arange(length // block, dtype=jnp.int32) * block
    return lax.map(one_block, starts).reshape(length, -1)

def per_head(operands):
    return head_span(operands[0], operands[1], operands[2], operands[3])

def grouped_sum(left, right, groups):
    width = left.shape[1] // groups
    total = jnp.zeros((left.shape[0], right.shape[1]), jnp.float32)
    for group in range(groups):
        partial_sum = jnp.dot(left[:, group * width:(group + 1) * width], right[group * width:(group + 1) * width], preferred_element_type=jnp.float32)
        rounded = lax.optimization_barrier(partial_sum.astype(jnp.bfloat16))
        total = total + rounded.astype(jnp.float32)
    return total

def one_expert(operands):
    rows_in, weight_gate, weight_up, weight_down = operands
    gate_part = jnp.dot(rows_in, weight_gate, preferred_element_type=jnp.float32)
    up_part = jnp.dot(rows_in, weight_up, preferred_element_type=jnp.float32)
    hidden = (jax.nn.silu(gate_part) * up_part).astype(jnp.bfloat16)
    return grouped_sum(hidden, weight_down, N_TP).astype(jnp.bfloat16)

def reference(queries, keys, values, key_bias, out_weight, moe_input, moe_gain, route_ids, route_scores, shared_gate, shared_up, shared_down, expert_gate, expert_up, expert_down):
    pieces = []
    for sequence_index in range(SEQUENCE_COUNT):
        first = sequence_index * SEQUENCE_LENGTH
        query_seq = queries[first:first + SEQUENCE_LENGTH].reshape(SEQUENCE_LENGTH, HEADS, HD).transpose(1, 0, 2)
        key_seq = keys[first:first + SEQUENCE_LENGTH].reshape(SEQUENCE_LENGTH, HEADS, HD).transpose(1, 0, 2)
        value_seq = values[first:first + SEQUENCE_LENGTH].reshape(SEQUENCE_LENGTH, HEADS, HD).transpose(1, 0, 2)
        bias_seq = key_bias[first:first + SEQUENCE_LENGTH].T
        head_outs = lax.map(per_head, (query_seq, key_seq, value_seq, bias_seq))
        pieces.append(head_outs.transpose(1, 0, 2).reshape(SEQUENCE_LENGTH, HEADS * HD))
    heads_out = jnp.concatenate(pieces, axis=0)
    mixed_tokens = grouped_sum(heads_out, out_weight, N_TP).astype(jnp.bfloat16)
    inputs = moe_input.astype(jnp.float32)
    normed = (inputs * lax.rsqrt(lax.optimization_barrier(jnp.mean(inputs * inputs, axis=-1, keepdims=True)) + EPS_NORM) * moe_gain.astype(jnp.float32)).astype(jnp.bfloat16)
    shared_hidden = (jax.nn.silu(jnp.dot(normed, shared_gate, preferred_element_type=jnp.float32)) * jnp.dot(normed, shared_up, preferred_element_type=jnp.float32)).astype(jnp.bfloat16)
    shared_result = grouped_sum(shared_hidden, shared_down, N_TP)
    chosen = route_ids.reshape(N_EP, ROWS_M * TOPK).astype(jnp.int32)
    onehot = (chosen[:, :, None] == jnp.arange(EXPERTS, dtype=jnp.int32)[None, None, :]).astype(jnp.int32)
    place = lax.optimization_barrier(jnp.sum((jnp.cumsum(onehot, axis=1) - onehot) * onehot, axis=2))
    block_ids = jnp.arange(N_EP, dtype=jnp.int32)[:, None]
    slot_index = (chosen * (N_EP * CAP) + block_ids * CAP + place).reshape(-1).astype(jnp.int32)
    token_index = jnp.arange(TOKENS_M * TOPK, dtype=jnp.int32) // TOPK
    expert_rows = jnp.zeros((EXPERTS * N_EP * CAP, D), jnp.bfloat16).at[slot_index].set(normed[token_index])
    expert_rows = expert_rows.reshape(EXPERTS, N_EP * CAP, D)
    results = lax.map(one_expert, (expert_rows, expert_gate, expert_up, expert_down))
    results = results.reshape(EXPERTS * N_EP * CAP, D)
    picked = results[slot_index].astype(jnp.float32).reshape(TOKENS_M, TOPK, D)
    scores = route_scores.astype(jnp.float32)
    gates = scores / lax.optimization_barrier(jnp.sum(scores, axis=-1, keepdims=True)) * ROUTED_SCALE
    expert_mix = (shared_result + lax.optimization_barrier(jnp.sum(gates[:, :, None] * picked, axis=1))).astype(jnp.bfloat16)
    return (mixed_tokens, expert_mix)
```

```python
import functools
import types

import jax
import jax.numpy as jnp
from jax import lax
from jax.experimental import pallas as pl
from jax.experimental.pallas import tpu as pltpu
from jax.sharding import PartitionSpec as P

EPS_NORM = 1e-06
ROUTED_SCALE = 2.5
LOG2E = 1.4426950408889634
MESH = pl.DeviceIdType.MESH
BF16 = jnp.bfloat16
F32 = jnp.float32
INPUTS = (
    "queries",
    "keys",
    "values",
    "bias",
    "out_w",
    "tokens",
    "gain",
    "ids",
    "scores",
    "sh_gate",
    "sh_up",
    "sh_down",
    "ex_gate",
    "ex_up",
    "ex_down",
)
OUTPUTS = ("mixed", "mix")


def columns(index, width):
    return pl.ds(pl.multiple_of(index * width, width), width)


def dot(left, right):
    return jnp.dot(left, right, preferred_element_type=F32)


class Plan:
    def __init__(self, ep, tp, queries, key_bias, moe_input, route_ids, expert_gate):
        self.ep, self.tp = ep, tp
        self.chips = tp // 2
        self.span = queries[0]
        self.heads = key_bias[1]
        self.size = queries[1] // self.heads
        self.half = ep // 2
        self.groups = self.half // self.heads
        self.share = self.span // self.groups
        self.sub = min(self.share, max(16, self.span // self.half))
        self.subs = self.share // self.sub
        self.width = min(256, self.span)
        self.tokens, self.features = moe_input
        self.col = self.features // tp
        self.topk = route_ids[1]
        self.experts = ep * expert_gate[0]
        capacity = 3 * self.tokens * self.topk // (2 * self.experts)
        self.cap = -(-capacity // 16) * 16
        self.slots = self.experts * self.cap
        self.hidden = expert_gate[2]
        self.rows = self.slots + self.tokens


def kernel(p, names, *refs):
    s = types.SimpleNamespace(**dict(zip(names, refs, strict=True)))
    ep, tp, half, heads, groups = p.ep, p.tp, p.half, p.heads, p.groups
    share, size, span, sub, subs = p.share, p.size, p.span, p.sub, p.subs
    own, own_tp = lax.axis_index("ep"), lax.axis_index("tp")
    side, loc = own // half, lax.rem(own, half)
    own_head, own_group = loc // groups, lax.rem(loc, groups)
    chip, core = own_tp // 2, lax.rem(own_tp, 2)
    beside = own_tp + 1 - 2 * core
    across = [lax.rem(chip + i, p.chips) for i in range(1, p.chips)]

    def remote(source, target, send, recv, axis, device):
        return pltpu.make_async_remote_copy(
            src_ref=source,
            dst_ref=target,
            send_sem=send,
            recv_sem=recv,
            device_id={axis: device},
            device_id_type=MESH,
        )

    def arrived(target, recv):
        remote(target, target, recv, recv, "tp", beside).wait_recv()

    sent = []

    def start(copy):
        copy.start()
        sent.append(copy)

    loads = []

    def load(source, target):
        copy = pltpu.make_async_copy(source, target, s.load.at[len(loads)])
        copy.start()
        loads.append(copy)
        return copy

    in_load = load(s.tokens, s.x_in)
    barrier = pltpu.get_barrier_semaphore()
    for i in range(1, ep):
        pl.semaphore_signal(
            barrier, inc=1, device_id={"ep": lax.rem(own + i, ep)}, device_id_type=MESH
        )
    for i in range(1, tp):
        pl.semaphore_signal(
            barrier, inc=1, device_id={"tp": lax.rem(own_tp + i, tp)}, device_id_type=MESH
        )
    bias = s.bias[...].astype(F32) * LOG2E
    for head in range(heads):
        s.b_stage[head] = jnp.broadcast_to(bias[head : head + 1, :], (8, span))
    index = lax.broadcasted_iota(jnp.int32, (p.width, p.width), 0)
    s.tri[...] = (index > lax.broadcasted_iota(jnp.int32, (p.width, p.width), 1)).astype(F32).astype(BF16)
    with jax.named_scope("enter"):
        pl.semaphore_wait(barrier, ep + tp - 2)

    def part(kind, head):
        if kind == 2:
            return s.b_stage.at[head]
        return (s.keys, s.values)[kind].at[:, columns(head, size)]

    part_outs = (s.k, s.v, s.b)

    def query_part(device):
        return s.queries.at[
            columns(lax.rem(device, groups), share), columns(device // groups, size)
        ]

    near = [lax.rem(loc + i, half) for i in range(1, half)]

    def send_part(kind):
        for other in near:
            start(
                remote(
                    part(kind, other // groups),
                    part_outs[kind].at[loc],
                    s.kv_send.at[kind, other],
                    s.kv_recv.at[kind, loc],
                    "ep",
                    side * half + other,
                )
            )

    kv_own = [
        pltpu.make_async_copy(part(kind, own_head), part_outs[kind].at[loc], s.kv_local.at[kind])
        for kind in range(3)
    ] + [pltpu.make_async_copy(query_part(loc), s.q.at[own], s.kv_local.at[3])]
    for copy in kv_own:
        copy.start()
    loads_shared = [load(s.sh_gate, s.w_sg), load(s.sh_up, s.w_su)]
    loads_expert = [load(s.ex_gate.at[0], s.w_eg), load(s.ex_up.at[0], s.w_eu)]

    with jax.named_scope("norm"):
        in_load.wait()
        inputs = s.x_in[...].astype(F32)
        normed = (
            inputs
            * lax.rsqrt(jnp.mean(inputs * inputs, axis=-1, keepdims=True) + EPS_NORM)
            * s.gain[...]
        ).astype(BF16)
        s.normed[...] = normed
        ids = s.ids[...]
        padded = -(-p.experts // 8) * 8
        expert = lax.broadcasted_iota(jnp.int32, (padded, p.tokens), 0)
        chosen = [(expert == ids[k : k + 1, :]).astype(F32) for k in range(p.topk)]
        named = chosen[0]
        for k in range(1, p.topk):
            named = named + chosen[k]
        before = (
            lax.broadcasted_iota(jnp.int32, (p.tokens, p.tokens), 0)
            < lax.broadcasted_iota(jnp.int32, (p.tokens, p.tokens), 1)
        ).astype(F32).astype(BF16)
        earlier = dot(named.astype(BF16), before)
        slot_row = lax.broadcasted_iota(jnp.int32, (p.slots, p.tokens), 0)
        slot_ids = []
        for k in range(p.topk):
            place = jnp.sum(chosen[k] * earlier, axis=0, keepdims=True).astype(jnp.int32)
            slot_ids.append(ids[k : k + 1, :] * p.cap + place)

        def table(weights):
            total = jnp.zeros((p.slots, p.tokens), F32)
            for k in range(p.topk):
                total = jnp.where(slot_row == slot_ids[k], weights[k], total)
            return total

        per = p.slots // ep
        ones = jnp.ones((1, p.tokens), F32)
        own_cols = s.normed[:, columns(own_tp, p.col)]
        outgoing = dot(table([ones] * p.topk).astype(BF16), own_cols).astype(BF16)
        s.rows_stage[...] = outgoing.reshape(ep, per, p.col)

    def grid_rows(device, slot):
        return s.grid.at[columns(device, per), columns(slot, p.col)]

    s.grid[columns(own, per), columns(own_tp, p.col)] = s.rows_stage[own]
    for i in range(1, ep):
        other = lax.rem(own + i, ep)
        start(
            remote(
                s.rows_stage.at[other],
                grid_rows(own, own_tp),
                s.rows_send.at[other],
                s.rows_recv.at[own],
                "ep",
                other,
            )
        )

    def far_query(device, piece, target):
        rows = pl.ds(lax.rem(target, groups) * share + piece * sub, sub)
        return remote(
            s.queries.at[rows, columns(target // groups, size)],
            s.q.at[half + device, pl.ds(piece * sub, sub)],
            s.q_send.at[half + target, piece],
            s.q_recv.at[half + device, piece],
            "ep",
            target,
        )

    def send_far(piece):
        @pl.when(side == 1)
        def _():
            for i in range(half):
                far_query(loc, piece, lax.rem(loc + i, half)).start()

    for kind in range(3):
        send_part(kind)
    send_far(0)
    for other in near:
        start(
            remote(
                query_part(other),
                s.q.at[own],
                s.q_send.at[other, 0],
                s.q_recv.at[loc, 0],
                "ep",
                side * half + other,
            )
        )
    for piece in range(1, subs):
        send_far(piece)

    def weight_pieces(number, source, target):
        for y in range(p.chips):
            load(source.at[:, columns(y * 2 + core, p.col)], target.at[core, y])
            start(
                remote(
                    source.at[:, columns(y * 2 + 1 - core, p.col)],
                    target.at[core, y],
                    s.w_send.at[number, y],
                    s.w_recv.at[number, y],
                    "tp",
                    beside,
                )
            )

    down_from = len(loads)
    weight_pieces(0, s.ex_down.at[0], s.w_ed)
    weight_pieces(1, s.sh_down, s.w_sd)
    weight_pieces(2, s.out_w, s.w_o)
    loads_down = loads[down_from:]

    tile = min(256, p.hidden)

    def gated(source, gate, up, first, count):
        def step(n, _):
            at = columns(n, tile)
            rows_in = source[...]
            left = dot(rows_in, gate[:, at])
            right = dot(rows_in, up[:, at])
            value = left / (1.0 + jnp.exp(-left)) * right
            s.hid[core, pl.ds(first, count), at] = value.astype(BF16)
            return 0

        lax.fori_loop(0, p.hidden // tile, step, 0)

    def swap_hidden(first, count, number):
        at = s.hid.at[core, pl.ds(first, count)]
        start(remote(at, at, s.hid_send.at[number], s.hid_recv.at[number], "tp", beside))

    with jax.named_scope("shared"):
        for copy in loads_shared:
            copy.wait()
        gated(s.normed, s.w_sg, s.w_su, p.slots, p.tokens)
        swap_hidden(p.slots, p.tokens, 1)

    sources = [lax.rem(own + ep - i, ep) for i in range(ep)]
    with jax.named_scope("rows_wait"):
        for source in sources:
            mine = grid_rows(source, own_tp)
            if source is not sources[0]:
                arrived(mine, s.rows_recv.at[source])
            for other in [y * 2 + core for y in across] + [beside]:
                start(
                    remote(
                        mine,
                        mine,
                        s.relay_send.at[source, other],
                        s.relay_recv.at[source, own_tp],
                        "tp",
                        other,
                    )
                )
    with jax.named_scope("relay_wait"):
        for source in sources:
            for y in across:
                slot = y * 2 + core
                piece = grid_rows(source, slot)
                arrived(piece, s.relay_recv.at[source, slot])
                start(
                    remote(
                        piece,
                        piece,
                        s.pass_send.at[source, slot],
                        s.relay_recv.at[source, slot],
                        "tp",
                        beside,
                    )
                )
        for source in sources:
            for y in [chip] + across:
                slot = y * 2 + 1 - core
                arrived(grid_rows(source, slot), s.relay_recv.at[source, slot])

    with jax.named_scope("expert"):
        for copy in loads_expert:
            copy.wait()
        gated(s.grid, s.w_eg, s.w_eu, 0, p.slots)
        swap_hidden(0, p.slots, 0)
    with jax.named_scope("swap_wait"):
        for copy in loads_down:
            copy.wait()
        for number, target in enumerate((s.w_ed, s.w_sd, s.w_o)):
            for y in range(p.chips):
                arrived(target.at[1 - core, y], s.w_recv.at[number, y])
        arrived(s.hid.at[1 - core, pl.ds(p.slots, p.tokens)], s.hid_recv.at[1])
        arrived(s.hid.at[1 - core, pl.ds(0, p.slots)], s.hid_recv.at[0])

    def down(y):
        routed = dot(s.hid[0, : p.slots], s.w_ed[0, y]) + dot(s.hid[1, : p.slots], s.w_ed[1, y])
        common = dot(s.hid[0, p.slots :], s.w_sd[0, y]) + dot(s.hid[1, p.slots :], s.w_sd[1, y])
        return routed, common

    with jax.named_scope("down"):
        for y in across:
            routed, common = down(y)
            s.part_send[y, : p.slots] = routed.astype(BF16)
            s.part_send[y, p.slots :] = common.astype(BF16)
            start(
                remote(
                    s.part_send.at[y],
                    s.part_recv.at[chip],
                    s.part_ssem.at[y],
                    s.part_rsem.at[chip],
                    "tp",
                    y * 2 + core,
                )
            )
        routed, common = down(chip)
        s.part_own[: p.slots] = routed
        s.part_own[p.slots :] = common

    scale = size ** (-0.5) * LOG2E

    def unit(query, block, carry, masked):
        count = query.shape[0]
        total, passed = carry
        key, value, bias_of = s.k[block], s.v[block], s.b[block]
        for first in range(span - p.width, -1, -p.width):
            logit = (
                lax.dot_general(
                    query,
                    key[first : first + p.width],
                    (((1,), (1,)), ((), ())),
                    preferred_element_type=F32,
                )
                * scale
                + bias_of[0:1, first : first + p.width]
            )
            drop = jnp.maximum(logit, jnp.log2(1.0 + jnp.exp2(jnp.minimum(logit, 126.0))))
            base = logit - drop
            if masked:
                shape = (count, p.width)
                visible = first + lax.broadcasted_iota(
                    jnp.int32, shape, 1
                ) < own_group * share + lax.broadcasted_iota(jnp.int32, shape, 0)
                drop = jnp.where(visible, drop, 0.0)
            later = dot(drop.astype(BF16), s.tri[...])
            weight = jnp.exp2(base - later - passed)
            if masked:
                weight = jnp.where(visible, weight, 0.0)
            passed = passed + later[:, 0:1] + drop[:, 0:1]
            total = total + dot(weight.astype(BF16), value[first : first + p.width])
        return total, passed

    def zeros(count):
        return jnp.zeros((count, size), F32), jnp.zeros((count, 1), F32)

    def heads_rows(piece, group):
        return pl.ds(pl.multiple_of((piece * groups + group) * sub, sub), sub)

    def out_piece(block, piece):
        return remote(
            s.o_stage.at[block, pl.ds(piece * sub, sub)],
            s.heads.at[core, heads_rows(piece, own_group), columns(own_head, size)],
            s.o_send.at[block, piece],
            s.o_recv.at[loc, piece],
            "ep",
            side * half + block,
        )

    def hand_on(block, piece):
        @pl.when(block != loc)
        def _():
            out_piece(block, piece).start()

        @pl.when(block == loc)
        def _():
            s.heads[core, heads_rows(piece, own_group), columns(own_head, size)] = s.o_stage[
                block, pl.ds(piece * sub, sub)
            ]

    def local_block(block, _):
        with jax.named_scope("q_wait"):

            @pl.when(block != loc)
            def _():
                arrived(s.q.at[side * half + block], s.q_recv.at[block, 0])

        with jax.named_scope("local"):
            query = s.q[side * half + block]
            carry = unit(query, block, zeros(share), True)
            carry = lax.fori_loop(
                0, block, lambda i, c: unit(query, block - 1 - i, c, False), carry
            )

        @pl.when(side == 0)
        def _():
            s.o_stage[block] = carry[0].astype(BF16)
            for piece in range(subs):
                hand_on(block, piece)

        @pl.when(side == 1)
        def _():
            s.o_part[block] = carry[0]
            s.passed[block] = jnp.broadcast_to(jnp.exp2(-carry[1]), (share, size))

        return 0

    with jax.named_scope("kv_wait"):
        for copy in kv_own:
            copy.wait()
        for block in range(half):

            @pl.when(block != loc)
            def _():
                for kind in range(3):
                    arrived(part_outs[kind].at[block], s.kv_recv.at[kind, block])


    def back_copy(other):
        return remote(
            s.back_stage.at[other],
            s.back.at[own],
            s.back_send.at[other],
            s.back_recv.at[own],
            "ep",
            other,
        )

    def give_back():
        with jax.named_scope("sums"):
            total = s.part_own[...]
            for y in across:
                arrived(s.part_recv.at[y], s.part_rsem.at[y])
                total = total + s.part_recv[y].astype(F32)
            s.part_own[...] = total
            s.back_stage[...] = total[: p.slots].astype(BF16).reshape(ep, per, p.col)
            s.back[own] = s.back_stage[own]
            for i in range(1, ep):
                other = lax.rem(own + i, ep)
                back_copy(other).start()

    def combine():
        with jax.named_scope("back_wait"):
            for i in range(1, ep):
                other = lax.rem(own + i, ep)
                arrived(s.back.at[other], s.back_recv.at[other])
        with jax.named_scope("combine"):
            scores = s.scores[...]
            score_sum = scores[0:1, :]
            for k in range(1, p.topk):
                score_sum = score_sum + scores[k : k + 1, :]
            gates = table(
                [scores[k : k + 1, :] / score_sum * ROUTED_SCALE for k in range(p.topk)]
            ).T
            high = gates.astype(BF16)
            low = (gates - high.astype(F32)).astype(BF16)
            returned = s.back[...].reshape(p.slots, p.col)
            s.mix[...] = (s.part_own[p.slots :] + dot(high, returned) + dot(low, returned)).astype(BF16)

    def out_rows(piece, count):
        return pl.ds(piece * groups * sub, count * groups * sub)

    def sibling(piece, count, slot):
        at = s.heads.at[slot, out_rows(piece, count)]
        return remote(at, at, s.sib_send.at[piece], s.sib_recv.at[piece], "tp", beside)

    def out_copy(y, piece, count):
        at = out_rows(piece, count)
        return remote(
            s.out_send.at[y, at],
            s.out_recv.at[chip, at],
            s.out_ssem.at[y, piece],
            s.out_rsem.at[chip, piece],
            "tp",
            y * 2 + core,
        )

    def project(piece, count):
        with jax.named_scope("o_wait"):
            for number in range(piece, piece + count):
                for source in range(half):

                    @pl.when(source != loc)
                    def _():
                        group, head = source % groups, source // groups
                        arrived(
                            s.heads.at[
                                core,
                                heads_rows(number, group),
                                pl.ds(head * size, size),
                            ],
                            s.o_recv.at[source, number],
                        )

        with jax.named_scope("sib_wait"):
            sibling(piece, count, core).start()
            sibling(piece, count, 1 - core).wait_recv()
        at = out_rows(piece, count)
        with jax.named_scope("proj"):
            for y in across:
                s.out_send[y, at] = (
                    dot(s.heads[0, at], s.w_o[0, y]) + dot(s.heads[1, at], s.w_o[1, y])
                ).astype(BF16)
                out_copy(y, piece, count).start()
            s.out_own[at] = dot(s.heads[0, at], s.w_o[0, chip]) + dot(s.heads[1, at], s.w_o[1, chip])

    def finish(piece, count):
        at = out_rows(piece, count)
        total = s.out_own[at]
        with jax.named_scope("out_wait"):
            for y in across:
                arrived(s.out_recv.at[y, at], s.out_rsem.at[y, piece])
                total = total + s.out_recv[y, at].astype(F32)
        total = total.astype(BF16)
        for number in range(piece, piece + count):
            for group in range(groups):
                first = ((number - piece) * groups + group) * sub
                s.mixed[pl.ds(group * share + number * sub, sub)] = total[first : first + sub]
        for y in across:
            out_copy(y, piece, count).wait_send()
        sibling(piece, count, core).wait_send()

    def mirror(piece):
        return remote(
            s.hl_stage.at[piece],
            s.hl.at[piece],
            s.hl_send.at[piece],
            s.hl_recv.at[piece],
            "ep",
            loc + half,
        )

    @pl.when(side == 0)
    def _():
        def far_tile(piece):
            with jax.named_scope("far_wait"):
                for block in range(half):
                    target = s.q.at[half + block, pl.ds(piece * sub, sub)]
                    arrived(target, s.q_recv.at[half + block, piece])
            with jax.named_scope("far"):
                query = s.q[half:, piece * sub : (piece + 1) * sub].reshape(half * sub, size)
                carry = lax.fori_loop(
                    0, half, lambda i, c: unit(query, half - 1 - i, c, False), zeros(half * sub)
                )
            s.hl_stage[piece] = carry[0].astype(BF16)
            mirror(piece).start()

        for piece in range(subs):
            far_tile(piece)
        give_back()
        lax.fori_loop(0, half, local_block, 0)
        project(0, subs)
        combine()
        finish(0, subs)
        for piece in range(subs):
            mirror(piece).wait_send()

    @pl.when(side == 1)
    def _():
        def merge(piece):
            with jax.named_scope("hl_wait"):
                arrived(s.hl.at[piece], s.hl_recv.at[piece])
            rows = slice(piece * sub, (piece + 1) * sub)
            s.o_stage[:, rows] = (
                s.o_part[:, rows]
                + s.passed[:, rows] * s.hl[piece].astype(F32).reshape(half, sub, size)
            ).astype(BF16)
            for block in range(half):
                hand_on(block, piece)

        lax.fori_loop(0, half, local_block, 0)
        give_back()
        merge(0)
        for piece in range(1, subs):
            merge(piece)
            project(piece - 1, 1)
        project(subs - 1, 1)
        for piece in range(subs - 1):
            finish(piece, 1)
        combine()
        finish(subs - 1, 1)
        for piece in range(subs):
            for i in range(half):
                far_query(loc, piece, lax.rem(loc + i, half)).wait_send()

    for i in range(1, ep):
        back_copy(lax.rem(own + i, ep)).wait_send()
    for block in range(half):

        @pl.when(block != loc)
        def _():
            for piece in range(subs):
                out_piece(block, piece).wait_send()

    for copy in sent:
        copy.wait_send()


def fused(p, *operands):
    dma = pltpu.SemaphoreType.DMA
    ep, tp, half, chips = p.ep, p.tp, p.half, p.chips
    per = p.slots // ep
    vmem = pl.BlockSpec(memory_space=pltpu.VMEM)
    free = pl.BlockSpec(memory_space=pl.ANY)
    small = ("bias", "gain", "ids", "scores")

    def buffer(shape, kind=BF16):
        return pltpu.VMEM(shape, kind)

    depth = p.heads * p.size
    scratch = {
        "q": buffer((ep, p.share, p.size)),
        "k": buffer((half, p.span, p.size)),
        "v": buffer((half, p.span, p.size)),
        "b": buffer((half, 8, p.span), F32),
        "b_stage": buffer((p.heads, 8, p.span), F32),
        "tri": buffer((p.width, p.width)),
        "hl_stage": buffer((p.subs, half * p.sub, p.size)),
        "hl": buffer((p.subs, half * p.sub, p.size)),
        "o_part": buffer((half, p.share, p.size), F32),
        "passed": buffer((half, p.share, p.size), F32),
        "o_stage": buffer((half, p.share, p.size)),
        "heads": buffer((2, p.span, depth)),
        "normed": buffer((p.tokens, p.features)),
        "rows_stage": buffer((ep, per, p.col)),
        "grid": buffer((p.slots, p.features)),
        "x_in": buffer((p.tokens, p.features)),
        "w_sg": buffer((p.features, p.hidden)),
        "w_su": buffer((p.features, p.hidden)),
        "w_eg": buffer((p.features, p.hidden)),
        "w_eu": buffer((p.features, p.hidden)),
        "w_sd": buffer((2, chips, p.hidden, p.col)),
        "w_ed": buffer((2, chips, p.hidden, p.col)),
        "w_o": buffer((2, chips, depth, p.col)),
        "hid": buffer((2, p.rows, p.hidden)),
        "part_send": buffer((chips, p.rows, p.col)),
        "part_recv": buffer((chips, p.rows, p.col)),
        "part_own": buffer((p.rows, p.col), F32),
        "back_stage": buffer((ep, per, p.col)),
        "back": buffer((ep, per, p.col)),
        "out_send": buffer((chips, p.span, p.col)),
        "out_recv": buffer((chips, p.span, p.col)),
        "out_own": buffer((p.span, p.col), F32),
        "load": dma((5 + 3 * chips,)),
        "kv_local": dma((4,)),
        "kv_send": dma((3, half)),
        "kv_recv": dma((3, half)),
        "q_send": dma((ep, p.subs)),
        "q_recv": dma((ep, p.subs)),
        "hl_send": dma((p.subs,)),
        "hl_recv": dma((p.subs,)),
        "o_send": dma((half, p.subs)),
        "o_recv": dma((half, p.subs)),
        "sib_send": dma((p.subs,)),
        "sib_recv": dma((p.subs,)),
        "w_send": dma((3, chips)),
        "w_recv": dma((3, chips)),
        "rows_send": dma((ep,)),
        "rows_recv": dma((ep,)),
        "relay_send": dma((ep, tp)),
        "relay_recv": dma((ep, tp)),
        "pass_send": dma((ep, tp)),
        "hid_send": dma((2,)),
        "hid_recv": dma((2,)),
        "part_ssem": dma((chips,)),
        "part_rsem": dma((chips,)),
        "back_send": dma((ep,)),
        "back_recv": dma((ep,)),
        "out_ssem": dma((chips, p.subs)),
        "out_rsem": dma((chips, p.subs)),
    }
    names = INPUTS + OUTPUTS + tuple(scratch)
    return pl.pallas_call(
        functools.partial(kernel, p, names),
        in_specs=[vmem if name in small else free for name in INPUTS],
        out_specs=[vmem, vmem],
        out_shape=[
            jax.ShapeDtypeStruct((p.span, p.col), BF16),
            jax.ShapeDtypeStruct((p.tokens, p.col), BF16),
        ],
        scratch_shapes=list(scratch.values()),
        compiler_params=pltpu.CompilerParams(
            collective_id=0, has_side_effects=True, vmem_limit_bytes=62 * 1024 * 1024
        ),
        name="fused",
    )(*operands)


def body(
    queries,
    keys,
    values,
    key_bias,
    out_weight,
    moe_input,
    moe_gain,
    route_ids,
    route_scores,
    shared_gate,
    shared_up,
    shared_down,
    expert_gate,
    expert_up,
    expert_down,
):
    p = Plan(
        lax.axis_size("ep"),
        lax.axis_size("tp"),
        queries.shape,
        key_bias.shape,
        moe_input.shape,
        route_ids.shape,
        expert_gate.shape,
    )
    return fused(
        p,
        queries,
        keys,
        values,
        key_bias.T,
        out_weight,
        moe_input,
        moe_gain.reshape(1, -1),
        route_ids.T,
        route_scores.T,
        shared_gate,
        shared_up,
        shared_down,
        expert_gate,
        expert_up,
        expert_down,
    )


def solution(mesh):
    return jax.shard_map(
        body,
        mesh=mesh,
        in_specs=(
            P("ep", "tp"),
            P("ep", "tp"),
            P("ep", "tp"),
            P("ep", "tp"),
            P("tp", None),
            P("ep", None),
            P(),
            P("ep", None),
            P("ep", None),
            P(None, "tp"),
            P(None, "tp"),
            P("tp", None),
            P("ep", None, "tp"),
            P("ep", None, "tp"),
            P("ep", "tp", None),
        ),
        out_specs=(P("ep", "tp"), P("ep", "tp")),
        check_vma=False,
    )
```

```python
import functools
import types

import jax
import jax.numpy as jnp
from jax import lax
from jax.experimental import pallas as pl
from jax.experimental.pallas import tpu as pltpu
from jax.sharding import PartitionSpec as P

EPS_NORM = 1e-06
ROUTED_SCALE = 2.5
LOG2E = 1.4426950408889634
MESH = pl.DeviceIdType.MESH
BF16 = jnp.bfloat16
F32 = jnp.float32
INPUTS = (
    "queries",
    "keys",
    "values",
    "bias",
    "out_w",
    "tokens",
    "gain",
    "ids",
    "scores",
    "sh_gate",
    "sh_up",
    "sh_down",
    "ex_gate",
    "ex_up",
    "ex_down",
)
OUTPUTS = ("mixed", "mix")


def columns(index, width):
    return pl.ds(pl.multiple_of(index * width, width), width)


def dot(left, right):
    return jnp.dot(left, right, preferred_element_type=F32)


class Plan:
    def __init__(self, ep, tp, queries, key_bias, moe_input, route_ids, expert_gate):
        self.ep, self.tp = ep, tp
        self.chips = tp // 2
        self.span = queries[0]
        self.heads = key_bias[1]
        self.size = queries[1] // self.heads
        self.half = ep // 2
        self.groups = self.half // self.heads
        self.share = self.span // self.groups
        self.sub = min(self.share, max(16, self.span // self.half))
        self.subs = self.share // self.sub
        self.width = min(256, self.span)
        self.tokens, self.features = moe_input
        self.col = self.features // tp
        self.topk = route_ids[1]
        self.experts = ep * expert_gate[0]
        capacity = 3 * self.tokens * self.topk // (2 * self.experts)
        self.cap = -(-capacity // 16) * 16
        self.slots = self.experts * self.cap
        self.hidden = expert_gate[2]
        self.rows = self.slots + self.tokens


def kernel(p, names, *refs):
    s = types.SimpleNamespace(**dict(zip(names, refs, strict=True)))
    ep, tp, half, heads, groups = p.ep, p.tp, p.half, p.heads, p.groups
    share, size, span, sub, subs = p.share, p.size, p.span, p.sub, p.subs
    own, own_tp = lax.axis_index("ep"), lax.axis_index("tp")
    side, loc = own // half, lax.rem(own, half)
    own_head, own_group = loc // groups, lax.rem(loc, groups)
    chip, core = own_tp // 2, lax.rem(own_tp, 2)
    beside = own_tp + 1 - 2 * core
    across = [lax.rem(chip + i, p.chips) for i in range(1, p.chips)]

    def remote(source, target, send, recv, axis, device):
        return pltpu.make_async_remote_copy(
            src_ref=source,
            dst_ref=target,
            send_sem=send,
            recv_sem=recv,
            device_id={axis: device},
            device_id_type=MESH,
        )

    def arrived(target, recv):
        remote(target, target, recv, recv, "tp", beside).wait_recv()

    sent = []

    def start(copy):
        copy.start()
        sent.append(copy)

    loads = []

    def load(source, target):
        copy = pltpu.make_async_copy(source, target, s.load.at[len(loads)])
        copy.start()
        loads.append(copy)
        return copy

    in_load = load(s.tokens, s.x_in)
    barrier = pltpu.get_barrier_semaphore()
    for i in range(1, ep):
        pl.semaphore_signal(
            barrier, inc=1, device_id={"ep": lax.rem(own + i, ep)}, device_id_type=MESH
        )
    for i in range(1, tp):
        pl.semaphore_signal(
            barrier, inc=1, device_id={"tp": lax.rem(own_tp + i, tp)}, device_id_type=MESH
        )
    bias = s.bias[...].astype(F32) * LOG2E
    for head in range(heads):
        s.b_stage[head] = jnp.broadcast_to(bias[head : head + 1, :], (8, span))
    index = lax.broadcasted_iota(jnp.int32, (p.width, p.width), 0)
    s.tri[...] = (index > lax.broadcasted_iota(jnp.int32, (p.width, p.width), 1)).astype(F32).astype(BF16)
    with jax.named_scope("enter"):
        pl.semaphore_wait(barrier, ep + tp - 2)

    def part(kind, head):
        if kind == 2:
            return s.b_stage.at[head]
        return (s.keys, s.values)[kind].at[:, columns(head, size)]

    part_outs = (s.k, s.v, s.b)

    def query_part(device):
        return s.queries.at[
            columns(lax.rem(device, groups), share), columns(device // groups, size)
        ]

    near = [lax.rem(loc + i, half) for i in range(1, half)]

    def send_part(kind):
        for other in near:
            start(
                remote(
                    part(kind, other // groups),
                    part_outs[kind].at[loc],
                    s.kv_send.at[kind, other],
                    s.kv_recv.at[kind, loc],
                    "ep",
                    side * half + other,
                )
            )

    kv_own = [
        pltpu.make_async_copy(part(kind, own_head), part_outs[kind].at[loc], s.kv_local.at[kind])
        for kind in range(3)
    ] + [pltpu.make_async_copy(query_part(loc), s.q.at[own], s.kv_local.at[3])]
    for copy in kv_own:
        copy.start()
    loads_shared = [load(s.sh_gate, s.w_sg), load(s.sh_up, s.w_su)]
    loads_expert = [load(s.ex_gate.at[0], s.w_eg), load(s.ex_up.at[0], s.w_eu)]

    with jax.named_scope("norm"):
        in_load.wait()
        inputs = s.x_in[...].astype(F32)
        normed = (
            inputs
            * lax.rsqrt(jnp.mean(inputs * inputs, axis=-1, keepdims=True) + EPS_NORM)
            * s.gain[...]
        ).astype(BF16)
        s.normed[...] = normed
        ids = s.ids[...]
        padded = -(-p.experts // 8) * 8
        expert = lax.broadcasted_iota(jnp.int32, (padded, p.tokens), 0)
        chosen = [(expert == ids[k : k + 1, :]).astype(F32) for k in range(p.topk)]
        named = chosen[0]
        for k in range(1, p.topk):
            named = named + chosen[k]
        before = (
            lax.broadcasted_iota(jnp.int32, (p.tokens, p.tokens), 0)
            < lax.broadcasted_iota(jnp.int32, (p.tokens, p.tokens), 1)
        ).astype(F32).astype(BF16)
        earlier = dot(named.astype(BF16), before)
        slot_row = lax.broadcasted_iota(jnp.int32, (p.slots, p.tokens), 0)
        slot_ids = []
        for k in range(p.topk):
            place = jnp.sum(chosen[k] * earlier, axis=0, keepdims=True).astype(jnp.int32)
            slot_ids.append(ids[k : k + 1, :] * p.cap + place)

        def table(weights):
            total = jnp.zeros((p.slots, p.tokens), F32)
            for k in range(p.topk):
                total = jnp.where(slot_row == slot_ids[k], weights[k], total)
            return total

        per = p.slots // ep
        ones = jnp.ones((1, p.tokens), F32)
        own_cols = s.normed[:, columns(own_tp, p.col)]
        outgoing = dot(table([ones] * p.topk).astype(BF16), own_cols).astype(BF16)
        s.rows_stage[...] = outgoing.reshape(ep, per, p.col)

    def grid_rows(device, slot):
        return s.grid.at[columns(device, per), columns(slot, p.col)]

    s.grid[columns(own, per), columns(own_tp, p.col)] = s.rows_stage[own]
    for i in range(1, ep):
        other = lax.rem(own + i, ep)
        start(
            remote(
                s.rows_stage.at[other],
                grid_rows(own, own_tp),
                s.rows_send.at[other],
                s.rows_recv.at[own],
                "ep",
                other,
            )
        )

    def far_query(device, piece, target):
        rows = pl.ds(lax.rem(target, groups) * share + piece * sub, sub)
        return remote(
            s.queries.at[rows, columns(target // groups, size)],
            s.q.at[half + device, pl.ds(piece * sub, sub)],
            s.q_send.at[half + target, piece],
            s.q_recv.at[half + device, piece],
            "ep",
            target,
        )

    def send_far(piece):
        @pl.when(side == 1)
        def _():
            for i in range(half):
                far_query(loc, piece, lax.rem(loc + i, half)).start()

    row = max(1, half // 2)

    def send_queries(same_row):
        for other in near:

            @pl.when((other // row == loc // row) == same_row)
            def _():
                remote(
                    query_part(other),
                    s.q.at[own],
                    s.q_send.at[other, 0],
                    s.q_recv.at[loc, 0],
                    "ep",
                    side * half + other,
                ).start()

    send_far(0)
    for kind in range(3):
        send_part(kind)
    send_queries(True)

    def weight_pieces(number, source, target):
        for y in range(p.chips):
            load(source.at[:, columns(y * 2 + core, p.col)], target.at[core, y])
            start(
                remote(
                    source.at[:, columns(y * 2 + 1 - core, p.col)],
                    target.at[core, y],
                    s.w_send.at[number, y],
                    s.w_recv.at[number, y],
                    "tp",
                    beside,
                )
            )

    down_from = len(loads)
    weight_pieces(0, s.ex_down.at[0], s.w_ed)
    weight_pieces(1, s.sh_down, s.w_sd)
    weight_pieces(2, s.out_w, s.w_o)
    loads_down = loads[down_from:]

    tile = min(256, p.hidden)

    def gated(source, gate, up, first, count):
        def step(n, _):
            at = columns(n, tile)
            rows_in = source[...]
            left = dot(rows_in, gate[:, at])
            right = dot(rows_in, up[:, at])
            value = left / (1.0 + jnp.exp(-left)) * right
            s.hid[core, pl.ds(first, count), at] = value.astype(BF16)
            return 0

        lax.fori_loop(0, p.hidden // tile, step, 0)

    def swap_hidden(first, count, number):
        at = s.hid.at[core, pl.ds(first, count)]
        start(remote(at, at, s.hid_send.at[number], s.hid_recv.at[number], "tp", beside))

    with jax.named_scope("shared"):
        for copy in loads_shared:
            copy.wait()
        gated(s.normed, s.w_sg, s.w_su, p.slots, p.tokens)
        swap_hidden(p.slots, p.tokens, 1)

    sources = [lax.rem(own + ep - i, ep) for i in range(ep)]
    with jax.named_scope("rows_wait"):
        for source in sources:
            mine = grid_rows(source, own_tp)
            if source is not sources[0]:
                arrived(mine, s.rows_recv.at[source])
            for other in [y * 2 + core for y in across] + [beside]:
                start(
                    remote(
                        mine,
                        mine,
                        s.relay_send.at[source, other],
                        s.relay_recv.at[source, own_tp],
                        "tp",
                        other,
                    )
                )
    with jax.named_scope("relay_wait"):
        for source in sources:
            for y in across:
                slot = y * 2 + core
                piece = grid_rows(source, slot)
                arrived(piece, s.relay_recv.at[source, slot])
                start(
                    remote(
                        piece,
                        piece,
                        s.pass_send.at[source, slot],
                        s.relay_recv.at[source, slot],
                        "tp",
                        beside,
                    )
                )
        for source in sources:
            for y in [chip] + across:
                slot = y * 2 + 1 - core
                arrived(grid_rows(source, slot), s.relay_recv.at[source, slot])

    for piece in range(1, min(3, subs)):
        send_far(piece)

    @pl.when(side == 1)
    def _():
        send_queries(False)

    with jax.named_scope("expert"):
        for copy in loads_expert:
            copy.wait()
        gated(s.grid, s.w_eg, s.w_eu, 0, p.slots)
        swap_hidden(0, p.slots, 0)
    with jax.named_scope("swap_wait"):
        for copy in loads_down:
            copy.wait()
        for number, target in enumerate((s.w_ed, s.w_sd, s.w_o)):
            for y in range(p.chips):
                arrived(target.at[1 - core, y], s.w_recv.at[number, y])
        arrived(s.hid.at[1 - core, pl.ds(p.slots, p.tokens)], s.hid_recv.at[1])
        arrived(s.hid.at[1 - core, pl.ds(0, p.slots)], s.hid_recv.at[0])

    def down(y):
        routed = dot(s.hid[0, : p.slots], s.w_ed[0, y]) + dot(s.hid[1, : p.slots], s.w_ed[1, y])
        common = dot(s.hid[0, p.slots :], s.w_sd[0, y]) + dot(s.hid[1, p.slots :], s.w_sd[1, y])
        return routed, common

    with jax.named_scope("down"):
        for y in across:
            routed, common = down(y)
            s.part_send[y, : p.slots] = routed.astype(BF16)
            s.part_send[y, p.slots :] = common.astype(BF16)
            start(
                remote(
                    s.part_send.at[y],
                    s.part_recv.at[chip],
                    s.part_ssem.at[y],
                    s.part_rsem.at[chip],
                    "tp",
                    y * 2 + core,
                )
            )
        routed, common = down(chip)
        s.part_own[: p.slots] = routed
        s.part_own[p.slots :] = common

    for piece in range(3, subs):
        send_far(piece)

    @pl.when(side == 0)
    def _():
        send_queries(False)

    scale = size ** (-0.5) * LOG2E

    def unit(query, block, carry, masked):
        count = query.shape[0]
        total, passed = carry
        key, value, bias_of = s.k[block], s.v[block], s.b[block]
        for first in range(span - p.width, -1, -p.width):
            logit = (
                lax.dot_general(
                    query,
                    key[first : first + p.width],
                    (((1,), (1,)), ((), ())),
                    preferred_element_type=F32,
                )
                * scale
                + bias_of[0:1, first : first + p.width]
            )
            drop = jnp.maximum(logit, jnp.log2(1.0 + jnp.exp2(jnp.minimum(logit, 126.0))))
            base = logit - drop
            if masked:
                shape = (count, p.width)
                visible = first + lax.broadcasted_iota(
                    jnp.int32, shape, 1
                ) < own_group * share + lax.broadcasted_iota(jnp.int32, shape, 0)
                drop = jnp.where(visible, drop, 0.0)
            later = dot(drop.astype(BF16), s.tri[...])
            weight = jnp.exp2(base - later - passed)
            if masked:
                weight = jnp.where(visible, weight, 0.0)
            passed = passed + later[:, 0:1] + drop[:, 0:1]
            total = total + dot(weight.astype(BF16), value[first : first + p.width])
        return total, passed

    def zeros(count):
        return jnp.zeros((count, size), F32), jnp.zeros((count, 1), F32)

    def heads_rows(piece, group):
        return pl.ds(pl.multiple_of((piece * groups + group) * sub, sub), sub)

    def out_piece(block, piece):
        return remote(
            s.o_stage.at[block, pl.ds(piece * sub, sub)],
            s.heads.at[core, heads_rows(piece, own_group), columns(own_head, size)],
            s.o_send.at[block, piece],
            s.o_recv.at[loc, piece],
            "ep",
            side * half + block,
        )

    def hand_on(block, piece):
        @pl.when(block != loc)
        def _():
            out_piece(block, piece).start()

        @pl.when(block == loc)
        def _():
            s.heads[core, heads_rows(piece, own_group), columns(own_head, size)] = s.o_stage[
                block, pl.ds(piece * sub, sub)
            ]

    def local_block(block, _):
        with jax.named_scope("q_wait"):

            @pl.when(block != loc)
            def _():
                arrived(s.q.at[side * half + block], s.q_recv.at[block, 0])

        with jax.named_scope("local"):
            query = s.q[side * half + block]
            carry = unit(query, block, zeros(share), True)
            carry = lax.fori_loop(
                0, block, lambda i, c: unit(query, block - 1 - i, c, False), carry
            )

        @pl.when(side == 0)
        def _():
            s.o_stage[block] = carry[0].astype(BF16)
            for piece in range(subs):
                hand_on(block, piece)

        @pl.when(side == 1)
        def _():
            s.o_part[block] = carry[0]
            s.passed[block] = jnp.broadcast_to(jnp.exp2(-carry[1]), (share, size))

        return 0

    def keys_arrive(blocks):
        with jax.named_scope("kv_wait"):
            for block in blocks:

                @pl.when(block == loc)
                def _():
                    for copy in kv_own:
                        copy.wait()

                @pl.when(block != loc)
                def _():
                    for kind in range(3):
                        arrived(part_outs[kind].at[block], s.kv_recv.at[kind, block])

    def back_copy(other):
        return remote(
            s.back_stage.at[other],
            s.back.at[own],
            s.back_send.at[other],
            s.back_recv.at[own],
            "ep",
            other,
        )

    def give_back():
        with jax.named_scope("sums"):
            total = s.part_own[...]
            for y in across:
                arrived(s.part_recv.at[y], s.part_rsem.at[y])
                total = total + s.part_recv[y].astype(F32)
            s.part_own[...] = total
            s.back_stage[...] = total[: p.slots].astype(BF16).reshape(ep, per, p.col)
            s.back[own] = s.back_stage[own]
            for i in range(1, ep):
                other = lax.rem(own + i, ep)
                back_copy(other).start()

    def combine():
        with jax.named_scope("back_wait"):
            for i in range(1, ep):
                other = lax.rem(own + i, ep)
                arrived(s.back.at[other], s.back_recv.at[other])
        with jax.named_scope("combine"):
            scores = s.scores[...]
            score_sum = scores[0:1, :]
            for k in range(1, p.topk):
                score_sum = score_sum + scores[k : k + 1, :]
            gates = table(
                [scores[k : k + 1, :] / score_sum * ROUTED_SCALE for k in range(p.topk)]
            ).T
            high = gates.astype(BF16)
            low = (gates - high.astype(F32)).astype(BF16)
            returned = s.back[...].reshape(p.slots, p.col)
            s.mix[...] = (s.part_own[p.slots :] + dot(high, returned) + dot(low, returned)).astype(BF16)

    def out_rows(piece, count):
        return pl.ds(piece * groups * sub, count * groups * sub)

    def sibling(piece, count, slot):
        at = s.heads.at[slot, out_rows(piece, count)]
        return remote(at, at, s.sib_send.at[piece], s.sib_recv.at[piece], "tp", beside)

    def out_copy(y, piece, count):
        at = out_rows(piece, count)
        return remote(
            s.out_send.at[y, at],
            s.out_recv.at[chip, at],
            s.out_ssem.at[y, piece],
            s.out_rsem.at[chip, piece],
            "tp",
            y * 2 + core,
        )

    def project(piece, count):
        with jax.named_scope("o_wait"):
            for number in range(piece, piece + count):
                for source in range(half):

                    @pl.when(source != loc)
                    def _():
                        group, head = source % groups, source // groups
                        arrived(
                            s.heads.at[
                                core,
                                heads_rows(number, group),
                                pl.ds(head * size, size),
                            ],
                            s.o_recv.at[source, number],
                        )

        with jax.named_scope("sib_wait"):
            sibling(piece, count, core).start()
            sibling(piece, count, 1 - core).wait_recv()
        at = out_rows(piece, count)
        with jax.named_scope("proj"):
            for y in across:
                s.out_send[y, at] = (
                    dot(s.heads[0, at], s.w_o[0, y]) + dot(s.heads[1, at], s.w_o[1, y])
                ).astype(BF16)
                out_copy(y, piece, count).start()
            s.out_own[at] = dot(s.heads[0, at], s.w_o[0, chip]) + dot(s.heads[1, at], s.w_o[1, chip])

    def finish(piece, count):
        at = out_rows(piece, count)
        total = s.out_own[at]
        with jax.named_scope("out_wait"):
            for y in across:
                arrived(s.out_recv.at[y, at], s.out_rsem.at[y, piece])
                total = total + s.out_recv[y, at].astype(F32)
        total = total.astype(BF16)
        for number in range(piece, piece + count):
            for group in range(groups):
                first = ((number - piece) * groups + group) * sub
                s.mixed[pl.ds(group * share + number * sub, sub)] = total[first : first + sub]
        for y in across:
            out_copy(y, piece, count).wait_send()
        sibling(piece, count, core).wait_send()

    def mirror(piece):
        return remote(
            s.hl_stage.at[piece],
            s.hl.at[piece],
            s.hl_send.at[piece],
            s.hl_recv.at[piece],
            "ep",
            loc + half,
        )

    @pl.when(side == 0)
    def _():
        def far_tile(piece):
            with jax.named_scope("far_wait"):
                for block in range(half):
                    target = s.q.at[half + block, pl.ds(piece * sub, sub)]
                    arrived(target, s.q_recv.at[half + block, piece])
            with jax.named_scope("far"):
                query = s.q[half:, piece * sub : (piece + 1) * sub].reshape(half * sub, size)
                carry = lax.fori_loop(
                    0, half, lambda i, c: unit(query, half - 1 - i, c, False), zeros(half * sub)
                )
            s.hl_stage[piece] = carry[0].astype(BF16)
            mirror(piece).start()

        first = jnp.where(loc < row, row, 0)
        keys_arrive(range(row))
        lax.fori_loop(0, first, local_block, 0)
        keys_arrive(range(row, half))
        ahead = max(1, subs // 2)
        for piece in range(ahead):
            far_tile(piece)
        lax.fori_loop(first, half, local_block, 0)
        for piece in range(ahead, subs):
            far_tile(piece)
        give_back()
        project(0, subs)
        combine()
        finish(0, subs)
        for piece in range(subs):
            mirror(piece).wait_send()

    @pl.when(side == 1)
    def _():
        def merge(piece):
            with jax.named_scope("hl_wait"):
                arrived(s.hl.at[piece], s.hl_recv.at[piece])
            rows = slice(piece * sub, (piece + 1) * sub)
            s.o_stage[:, rows] = (
                s.o_part[:, rows]
                + s.passed[:, rows] * s.hl[piece].astype(F32).reshape(half, sub, size)
            ).astype(BF16)
            for block in range(half):
                hand_on(block, piece)

        keys_arrive(range(half))
        lax.fori_loop(0, half, local_block, 0)
        give_back()
        merge(0)
        for piece in range(1, subs):
            merge(piece)
            project(piece - 1, 1)
        project(subs - 1, 1)
        for piece in range(subs - 1):
            finish(piece, 1)
        combine()
        finish(subs - 1, 1)
        for piece in range(subs):
            for i in range(half):
                far_query(loc, piece, lax.rem(loc + i, half)).wait_send()

    for i in range(1, ep):
        back_copy(lax.rem(own + i, ep)).wait_send()
    for block in range(half):

        @pl.when(block != loc)
        def _():
            for piece in range(subs):
                out_piece(block, piece).wait_send()

    for other in near:
        remote(
            query_part(other),
            s.q.at[own],
            s.q_send.at[other, 0],
            s.q_recv.at[loc, 0],
            "ep",
            side * half + other,
        ).wait_send()
    for copy in sent:
        copy.wait_send()


def fused(p, *operands):
    dma = pltpu.SemaphoreType.DMA
    ep, tp, half, chips = p.ep, p.tp, p.half, p.chips
    per = p.slots // ep
    vmem = pl.BlockSpec(memory_space=pltpu.VMEM)
    free = pl.BlockSpec(memory_space=pl.ANY)
    small = ("bias", "gain", "ids", "scores")

    def buffer(shape, kind=BF16):
        return pltpu.VMEM(shape, kind)

    depth = p.heads * p.size
    scratch = {
        "q": buffer((ep, p.share, p.size)),
        "k": buffer((half, p.span, p.size)),
        "v": buffer((half, p.span, p.size)),
        "b": buffer((half, 8, p.span), F32),
        "b_stage": buffer((p.heads, 8, p.span), F32),
        "tri": buffer((p.width, p.width)),
        "hl_stage": buffer((p.subs, half * p.sub, p.size)),
        "hl": buffer((p.subs, half * p.sub, p.size)),
        "o_part": buffer((half, p.share, p.size), F32),
        "passed": buffer((half, p.share, p.size), F32),
        "o_stage": buffer((half, p.share, p.size)),
        "heads": buffer((2, p.span, depth)),
        "normed": buffer((p.tokens, p.features)),
        "rows_stage": buffer((ep, per, p.col)),
        "grid": buffer((p.slots, p.features)),
        "x_in": buffer((p.tokens, p.features)),
        "w_sg": buffer((p.features, p.hidden)),
        "w_su": buffer((p.features, p.hidden)),
        "w_eg": buffer((p.features, p.hidden)),
        "w_eu": buffer((p.features, p.hidden)),
        "w_sd": buffer((2, chips, p.hidden, p.col)),
        "w_ed": buffer((2, chips, p.hidden, p.col)),
        "w_o": buffer((2, chips, depth, p.col)),
        "hid": buffer((2, p.rows, p.hidden)),
        "part_send": buffer((chips, p.rows, p.col)),
        "part_recv": buffer((chips, p.rows, p.col)),
        "part_own": buffer((p.rows, p.col), F32),
        "back_stage": buffer((ep, per, p.col)),
        "back": buffer((ep, per, p.col)),
        "out_send": buffer((chips, p.span, p.col)),
        "out_recv": buffer((chips, p.span, p.col)),
        "out_own": buffer((p.span, p.col), F32),
        "load": dma((5 + 3 * chips,)),
        "kv_local": dma((4,)),
        "kv_send": dma((3, half)),
        "kv_recv": dma((3, half)),
        "q_send": dma((ep, p.subs)),
        "q_recv": dma((ep, p.subs)),
        "hl_send": dma((p.subs,)),
        "hl_recv": dma((p.subs,)),
        "o_send": dma((half, p.subs)),
        "o_recv": dma((half, p.subs)),
        "sib_send": dma((p.subs,)),
        "sib_recv": dma((p.subs,)),
        "w_send": dma((3, chips)),
        "w_recv": dma((3, chips)),
        "rows_send": dma((ep,)),
        "rows_recv": dma((ep,)),
        "relay_send": dma((ep, tp)),
        "relay_recv": dma((ep, tp)),
        "pass_send": dma((ep, tp)),
        "hid_send": dma((2,)),
        "hid_recv": dma((2,)),
        "part_ssem": dma((chips,)),
        "part_rsem": dma((chips,)),
        "back_send": dma((ep,)),
        "back_recv": dma((ep,)),
        "out_ssem": dma((chips, p.subs)),
        "out_rsem": dma((chips, p.subs)),
    }
    names = INPUTS + OUTPUTS + tuple(scratch)
    return pl.pallas_call(
        functools.partial(kernel, p, names),
        in_specs=[vmem if name in small else free for name in INPUTS],
        out_specs=[vmem, vmem],
        out_shape=[
            jax.ShapeDtypeStruct((p.span, p.col), BF16),
            jax.ShapeDtypeStruct((p.tokens, p.col), BF16),
        ],
        scratch_shapes=list(scratch.values()),
        compiler_params=pltpu.CompilerParams(
            collective_id=0, has_side_effects=True, vmem_limit_bytes=62 * 1024 * 1024
        ),
        name="fused",
    )(*operands)


def settle_kernel(mixed_in, mix_in, mixed_out, mix_out):
    mixed_out[...] = mixed_in[...]
    mix_out[...] = mix_in[...]


def settle(mixed, mix):
    vmem = pl.BlockSpec(memory_space=pltpu.VMEM)
    return pl.pallas_call(
        settle_kernel,
        in_specs=[vmem, vmem],
        out_specs=[vmem, vmem],
        out_shape=[jax.ShapeDtypeStruct(x.shape, x.dtype) for x in (mixed, mix)],
        name="settle",
    )(mixed, mix)


def body(
    queries,
    keys,
    values,
    key_bias,
    out_weight,
    moe_input,
    moe_gain,
    route_ids,
    route_scores,
    shared_gate,
    shared_up,
    shared_down,
    expert_gate,
    expert_up,
    expert_down,
):
    p = Plan(
        lax.axis_size("ep"),
        lax.axis_size("tp"),
        queries.shape,
        key_bias.shape,
        moe_input.shape,
        route_ids.shape,
        expert_gate.shape,
    )
    mixed, mix = fused(
        p,
        queries,
        keys,
        values,
        key_bias.T,
        out_weight,
        moe_input,
        moe_gain.reshape(1, -1),
        route_ids.T,
        route_scores.T,
        shared_gate,
        shared_up,
        shared_down,
        expert_gate,
        expert_up,
        expert_down,
    )
    return settle(mixed, mix)


def solution(mesh):
    return jax.shard_map(
        body,
        mesh=mesh,
        in_specs=(
            P("ep", "tp"),
            P("ep", "tp"),
            P("ep", "tp"),
            P("ep", "tp"),
            P("tp", None),
            P("ep", None),
            P(),
            P("ep", None),
            P("ep", None),
            P(None, "tp"),
            P(None, "tp"),
            P("tp", None),
            P("ep", None, "tp"),
            P("ep", None, "tp"),
            P("ep", "tp", None),
        ),
        out_specs=(P("ep", "tp"), P("ep", "tp")),
        check_vma=False,
    )
```

```python
import functools
import types

import jax
import jax.numpy as jnp
from jax import lax
from jax.experimental import pallas as pl
from jax.experimental.pallas import tpu as pltpu
from jax.sharding import PartitionSpec as P

EPS_NORM = 1e-06
ROUTED_SCALE = 2.5
LOG2E = 1.4426950408889634
MESH = pl.DeviceIdType.MESH
BF16 = jnp.bfloat16
F32 = jnp.float32
INPUTS = (
    "queries",
    "keys",
    "values",
    "bias",
    "out_w",
    "tokens",
    "gain",
    "ids",
    "scores",
    "sh_gate",
    "sh_up",
    "sh_down",
    "ex_gate",
    "ex_up",
    "ex_down",
)
OUTPUTS = ("mixed", "mix")


def columns(index, width):
    return pl.ds(pl.multiple_of(index * width, width), width)


def dot(left, right):
    return jnp.dot(left, right, preferred_element_type=F32)


class Plan:
    def __init__(self, ep, tp, queries, key_bias, moe_input, route_ids, expert_gate):
        self.ep, self.tp = ep, tp
        self.chips = tp // 2
        self.span = queries[0]
        self.heads = key_bias[1]
        self.size = queries[1] // self.heads
        self.half = ep // 2
        self.groups = self.half // self.heads
        self.share = self.span // self.groups
        self.sub = min(self.share, max(16, self.span // self.half))
        self.subs = self.share // self.sub
        self.width = min(256, self.span)
        self.tokens, self.features = moe_input
        self.col = self.features // tp
        self.topk = route_ids[1]
        self.experts = ep * expert_gate[0]
        capacity = 3 * self.tokens * self.topk // (2 * self.experts)
        self.cap = -(-capacity // 16) * 16
        self.slots = self.experts * self.cap
        self.hidden = expert_gate[2]
        self.rows = self.slots + self.tokens


def kernel(p, names, *refs):
    s = types.SimpleNamespace(**dict(zip(names, refs, strict=True)))
    ep, tp, half, heads, groups = p.ep, p.tp, p.half, p.heads, p.groups
    share, size, span, sub, subs = p.share, p.size, p.span, p.sub, p.subs
    own, own_tp = lax.axis_index("ep"), lax.axis_index("tp")
    side, loc = own // half, lax.rem(own, half)
    own_head, own_group = loc // groups, lax.rem(loc, groups)
    chip, core = own_tp // 2, lax.rem(own_tp, 2)
    beside = own_tp + 1 - 2 * core
    across = [lax.rem(chip + i, p.chips) for i in range(1, p.chips)]

    def remote(source, target, send, recv, axis, device):
        return pltpu.make_async_remote_copy(
            src_ref=source,
            dst_ref=target,
            send_sem=send,
            recv_sem=recv,
            device_id={axis: device},
            device_id_type=MESH,
        )

    def arrived(target, recv):
        remote(target, target, recv, recv, "tp", beside).wait_recv()

    sent = []

    def start(copy):
        copy.start()
        sent.append(copy)

    loads = []

    def load(source, target):
        copy = pltpu.make_async_copy(source, target, s.load.at[len(loads)])
        copy.start()
        loads.append(copy)
        return copy

    in_load = load(s.tokens, s.x_in)
    barrier = pltpu.get_barrier_semaphore()
    for i in range(1, ep):
        pl.semaphore_signal(
            barrier, inc=1, device_id={"ep": lax.rem(own + i, ep)}, device_id_type=MESH
        )
    for i in range(1, tp):
        pl.semaphore_signal(
            barrier, inc=1, device_id={"tp": lax.rem(own_tp + i, tp)}, device_id_type=MESH
        )
    bias = s.bias[...].astype(F32) * LOG2E
    for head in range(heads):
        s.b_stage[head] = jnp.broadcast_to(bias[head : head + 1, :], (8, span))
    index = lax.broadcasted_iota(jnp.int32, (p.width, p.width), 0)
    s.tri[...] = (index > lax.broadcasted_iota(jnp.int32, (p.width, p.width), 1)).astype(F32).astype(BF16)
    with jax.named_scope("enter"):
        pl.semaphore_wait(barrier, ep + tp - 2)

    def part(kind, head):
        if kind == 2:
            return s.b_stage.at[head]
        return (s.keys, s.values)[kind].at[:, columns(head, size)]

    part_outs = (s.k, s.v, s.b)

    def query_part(device):
        return s.queries.at[
            columns(lax.rem(device, groups), share), columns(device // groups, size)
        ]

    near = [lax.rem(loc + i, half) for i in range(1, half)]

    def send_part(kind):
        for other in near:
            start(
                remote(
                    part(kind, other // groups),
                    part_outs[kind].at[loc],
                    s.kv_send.at[kind, other],
                    s.kv_recv.at[kind, loc],
                    "ep",
                    side * half + other,
                )
            )

    kv_own = [
        pltpu.make_async_copy(part(kind, own_head), part_outs[kind].at[loc], s.kv_local.at[kind])
        for kind in range(3)
    ] + [pltpu.make_async_copy(query_part(loc), s.q.at[own], s.kv_local.at[3])]
    for copy in kv_own:
        copy.start()
    loads_shared = [load(s.sh_gate, s.w_sg), load(s.sh_up, s.w_su)]
    loads_expert = [load(s.ex_gate.at[0], s.w_eg), load(s.ex_up.at[0], s.w_eu)]

    with jax.named_scope("norm"):
        in_load.wait()
        inputs = s.x_in[...].astype(F32)
        normed = (
            inputs
            * lax.rsqrt(jnp.mean(inputs * inputs, axis=-1, keepdims=True) + EPS_NORM)
            * s.gain[...]
        ).astype(BF16)
        s.normed[...] = normed
        ids = s.ids[...]
        padded = -(-p.experts // 8) * 8
        expert = lax.broadcasted_iota(jnp.int32, (padded, p.tokens), 0)
        chosen = [(expert == ids[k : k + 1, :]).astype(F32) for k in range(p.topk)]
        named = chosen[0]
        for k in range(1, p.topk):
            named = named + chosen[k]
        before = (
            lax.broadcasted_iota(jnp.int32, (p.tokens, p.tokens), 0)
            < lax.broadcasted_iota(jnp.int32, (p.tokens, p.tokens), 1)
        ).astype(F32).astype(BF16)
        earlier = dot(named.astype(BF16), before)
        slot_row = lax.broadcasted_iota(jnp.int32, (p.slots, p.tokens), 0)
        slot_ids = []
        for k in range(p.topk):
            place = jnp.sum(chosen[k] * earlier, axis=0, keepdims=True).astype(jnp.int32)
            slot_ids.append(ids[k : k + 1, :] * p.cap + place)

        def table(weights):
            total = jnp.zeros((p.slots, p.tokens), F32)
            for k in range(p.topk):
                total = jnp.where(slot_row == slot_ids[k], weights[k], total)
            return total

        per = p.slots // ep
        ones = jnp.ones((1, p.tokens), F32)
        own_cols = s.normed[:, columns(own_tp, p.col)]
        outgoing = dot(table([ones] * p.topk).astype(BF16), own_cols).astype(BF16)
        s.rows_stage[...] = outgoing.reshape(ep, per, p.col)

    def grid_rows(device, slot):
        return s.grid.at[columns(device, per), columns(slot, p.col)]

    s.grid[columns(own, per), columns(own_tp, p.col)] = s.rows_stage[own]
    for i in range(1, ep):
        other = lax.rem(own + i, ep)
        start(
            remote(
                s.rows_stage.at[other],
                grid_rows(own, own_tp),
                s.rows_send.at[other],
                s.rows_recv.at[own],
                "ep",
                other,
            )
        )

    def far_query(device, piece, target):
        rows = pl.ds(lax.rem(target, groups) * share + piece * sub, sub)
        return remote(
            s.queries.at[rows, columns(target // groups, size)],
            s.q.at[half + device, pl.ds(piece * sub, sub)],
            s.q_send.at[half + target, piece],
            s.q_recv.at[half + device, piece],
            "ep",
            target,
        )

    def send_far(piece):
        @pl.when(side == 1)
        def _():
            for i in range(half):
                far_query(loc, piece, lax.rem(loc + i, half)).start()

    row = max(1, half // 2)

    def send_queries(same_row):
        for other in near:

            @pl.when((other // row == loc // row) == same_row)
            def _():
                remote(
                    query_part(other),
                    s.q.at[own],
                    s.q_send.at[other, 0],
                    s.q_recv.at[loc, 0],
                    "ep",
                    side * half + other,
                ).start()

    send_far(0)
    for kind in range(3):
        send_part(kind)
    send_queries(True)

    def weight_pieces(number, source, target):
        for y in range(p.chips):
            load(source.at[:, columns(y * 2 + core, p.col)], target.at[core, y])
            start(
                remote(
                    source.at[:, columns(y * 2 + 1 - core, p.col)],
                    target.at[core, y],
                    s.w_send.at[number, y],
                    s.w_recv.at[number, y],
                    "tp",
                    beside,
                )
            )

    down_from = len(loads)
    weight_pieces(0, s.ex_down.at[0], s.w_ed)
    weight_pieces(1, s.sh_down, s.w_sd)
    weight_pieces(2, s.out_w, s.w_o)
    loads_down = loads[down_from:]

    tile = min(256, p.hidden)

    def gated(source, gate, up, first, count):
        def step(n, _):
            at = columns(n, tile)
            rows_in = source[...]
            left = dot(rows_in, gate[:, at])
            right = dot(rows_in, up[:, at])
            value = left / (1.0 + jnp.exp(-left)) * right
            s.hid[core, pl.ds(first, count), at] = value.astype(BF16)
            return 0

        lax.fori_loop(0, p.hidden // tile, step, 0)

    def swap_hidden(first, count, number):
        at = s.hid.at[core, pl.ds(first, count)]
        start(remote(at, at, s.hid_send.at[number], s.hid_recv.at[number], "tp", beside))

    with jax.named_scope("shared"):
        for copy in loads_shared:
            copy.wait()
        gated(s.normed, s.w_sg, s.w_su, p.slots, p.tokens)
        swap_hidden(p.slots, p.tokens, 1)

    sources = [lax.rem(own + ep - i, ep) for i in range(ep)]
    with jax.named_scope("rows_wait"):
        for source in sources:
            mine = grid_rows(source, own_tp)
            if source is not sources[0]:
                arrived(mine, s.rows_recv.at[source])
            for other in [y * 2 + core for y in across] + [beside]:
                start(
                    remote(
                        mine,
                        mine,
                        s.relay_send.at[source, other],
                        s.relay_recv.at[source, own_tp],
                        "tp",
                        other,
                    )
                )
    with jax.named_scope("relay_wait"):
        for source in sources:
            for y in across:
                slot = y * 2 + core
                piece = grid_rows(source, slot)
                arrived(piece, s.relay_recv.at[source, slot])
                start(
                    remote(
                        piece,
                        piece,
                        s.pass_send.at[source, slot],
                        s.relay_recv.at[source, slot],
                        "tp",
                        beside,
                    )
                )
        for source in sources:
            for y in [chip] + across:
                slot = y * 2 + 1 - core
                arrived(grid_rows(source, slot), s.relay_recv.at[source, slot])

    if subs > 1:
        send_far(1)

    send_queries(False)

    with jax.named_scope("expert"):
        for copy in loads_expert:
            copy.wait()
        gated(s.grid, s.w_eg, s.w_eu, 0, p.slots)
        swap_hidden(0, p.slots, 0)
    with jax.named_scope("swap_wait"):
        for copy in loads_down:
            copy.wait()
        for number, target in enumerate((s.w_ed, s.w_sd, s.w_o)):
            for y in range(p.chips):
                arrived(target.at[1 - core, y], s.w_recv.at[number, y])
        arrived(s.hid.at[1 - core, pl.ds(p.slots, p.tokens)], s.hid_recv.at[1])
        arrived(s.hid.at[1 - core, pl.ds(0, p.slots)], s.hid_recv.at[0])

    def down(y):
        routed = dot(s.hid[0, : p.slots], s.w_ed[0, y]) + dot(s.hid[1, : p.slots], s.w_ed[1, y])
        common = dot(s.hid[0, p.slots :], s.w_sd[0, y]) + dot(s.hid[1, p.slots :], s.w_sd[1, y])
        return routed, common

    with jax.named_scope("down"):
        for y in across:
            routed, common = down(y)
            s.part_send[y, : p.slots] = routed.astype(BF16)
            s.part_send[y, p.slots :] = common.astype(BF16)
            start(
                remote(
                    s.part_send.at[y],
                    s.part_recv.at[chip],
                    s.part_ssem.at[y],
                    s.part_rsem.at[chip],
                    "tp",
                    y * 2 + core,
                )
            )
        routed, common = down(chip)
        s.part_own[: p.slots] = routed
        s.part_own[p.slots :] = common

    scale = size ** (-0.5) * LOG2E

    def unit(query, block, carry, masked):
        count = query.shape[0]
        total, passed = carry
        key, value, bias_of = s.k[block], s.v[block], s.b[block]
        for first in range(span - p.width, -1, -p.width):
            logit = (
                lax.dot_general(
                    query,
                    key[first : first + p.width],
                    (((1,), (1,)), ((), ())),
                    preferred_element_type=F32,
                )
                * scale
                + bias_of[0:1, first : first + p.width]
            )
            drop = jnp.maximum(logit, jnp.log2(1.0 + jnp.exp2(jnp.minimum(logit, 126.0))))
            base = logit - drop
            if masked:
                shape = (count, p.width)
                visible = first + lax.broadcasted_iota(
                    jnp.int32, shape, 1
                ) < own_group * share + lax.broadcasted_iota(jnp.int32, shape, 0)
                drop = jnp.where(visible, drop, 0.0)
            later = dot(drop.astype(BF16), s.tri[...])
            weight = jnp.exp2(base - later - passed)
            if masked:
                weight = jnp.where(visible, weight, 0.0)
            passed = passed + later[:, 0:1] + drop[:, 0:1]
            total = total + dot(weight.astype(BF16), value[first : first + p.width])
        return total, passed

    def zeros(count):
        return jnp.zeros((count, size), F32), jnp.zeros((count, 1), F32)

    def heads_rows(piece, group):
        return pl.ds(pl.multiple_of((piece * groups + group) * sub, sub), sub)

    def out_piece(block, piece):
        return remote(
            s.o_stage.at[block, pl.ds(piece * sub, sub)],
            s.heads.at[core, heads_rows(piece, own_group), columns(own_head, size)],
            s.o_send.at[block, piece],
            s.o_recv.at[loc, piece],
            "ep",
            side * half + block,
        )

    def hand_on(block, piece):
        @pl.when(block != loc)
        def _():
            out_piece(block, piece).start()

        @pl.when(block == loc)
        def _():
            s.heads[core, heads_rows(piece, own_group), columns(own_head, size)] = s.o_stage[
                block, pl.ds(piece * sub, sub)
            ]

    def local_block(block, _):
        with jax.named_scope("q_wait"):

            @pl.when(block != loc)
            def _():
                arrived(s.q.at[side * half + block], s.q_recv.at[block, 0])

        with jax.named_scope("local"):
            query = s.q[side * half + block]
            carry = unit(query, block, zeros(share), True)
            carry = lax.fori_loop(
                0, block, lambda i, c: unit(query, block - 1 - i, c, False), carry
            )

        @pl.when(side == 0)
        def _():
            s.o_stage[block] = carry[0].astype(BF16)
            for piece in range(subs):
                hand_on(block, piece)

        @pl.when(side == 1)
        def _():
            s.o_part[block] = carry[0]
            s.passed[block] = jnp.broadcast_to(jnp.exp2(-carry[1]), (share, size))

        return 0

    def keys_arrive(blocks):
        with jax.named_scope("kv_wait"):
            for block in blocks:

                @pl.when(block == loc)
                def _():
                    for copy in kv_own:
                        copy.wait()

                @pl.when(block != loc)
                def _():
                    for kind in range(3):
                        arrived(part_outs[kind].at[block], s.kv_recv.at[kind, block])

    def back_copy(other):
        return remote(
            s.back_stage.at[other],
            s.back.at[own],
            s.back_send.at[other],
            s.back_recv.at[own],
            "ep",
            other,
        )

    def give_back():
        with jax.named_scope("sums"):
            total = s.part_own[...]
            for y in across:
                arrived(s.part_recv.at[y], s.part_rsem.at[y])
                total = total + s.part_recv[y].astype(F32)
            s.part_own[...] = total
            s.back_stage[...] = total[: p.slots].astype(BF16).reshape(ep, per, p.col)
            s.back[own] = s.back_stage[own]
            for i in range(1, ep):
                other = lax.rem(own + i, ep)
                back_copy(other).start()

    def combine():
        with jax.named_scope("back_wait"):
            for i in range(1, ep):
                other = lax.rem(own + i, ep)
                arrived(s.back.at[other], s.back_recv.at[other])
        with jax.named_scope("combine"):
            scores = s.scores[...]
            score_sum = scores[0:1, :]
            for k in range(1, p.topk):
                score_sum = score_sum + scores[k : k + 1, :]
            gates = table(
                [scores[k : k + 1, :] / score_sum * ROUTED_SCALE for k in range(p.topk)]
            ).T
            high = gates.astype(BF16)
            low = (gates - high.astype(F32)).astype(BF16)
            returned = s.back[...].reshape(p.slots, p.col)
            s.mix[...] = (s.part_own[p.slots :] + dot(high, returned) + dot(low, returned)).astype(BF16)

    def out_rows(piece, count):
        return pl.ds(piece * groups * sub, count * groups * sub)

    def sibling(piece, count, slot):
        at = s.heads.at[slot, out_rows(piece, count)]
        return remote(at, at, s.sib_send.at[piece], s.sib_recv.at[piece], "tp", beside)

    def out_copy(y, piece, count):
        at = out_rows(piece, count)
        return remote(
            s.out_send.at[y, at],
            s.out_recv.at[chip, at],
            s.out_ssem.at[y, piece],
            s.out_rsem.at[chip, piece],
            "tp",
            y * 2 + core,
        )

    def project(piece, count):
        with jax.named_scope("o_wait"):
            for number in range(piece, piece + count):
                for source in range(half):

                    @pl.when(source != loc)
                    def _():
                        group, head = source % groups, source // groups
                        arrived(
                            s.heads.at[
                                core,
                                heads_rows(number, group),
                                pl.ds(head * size, size),
                            ],
                            s.o_recv.at[source, number],
                        )

        with jax.named_scope("sib_wait"):
            sibling(piece, count, core).start()
            sibling(piece, count, 1 - core).wait_recv()
        at = out_rows(piece, count)
        with jax.named_scope("proj"):
            for y in across:
                s.out_send[y, at] = (
                    dot(s.heads[0, at], s.w_o[0, y]) + dot(s.heads[1, at], s.w_o[1, y])
                ).astype(BF16)
                out_copy(y, piece, count).start()
            s.out_own[at] = dot(s.heads[0, at], s.w_o[0, chip]) + dot(s.heads[1, at], s.w_o[1, chip])

    def finish(piece, count):
        at = out_rows(piece, count)
        total = s.out_own[at]
        with jax.named_scope("out_wait"):
            for y in across:
                arrived(s.out_recv.at[y, at], s.out_rsem.at[y, piece])
                total = total + s.out_recv[y, at].astype(F32)
        total = total.astype(BF16)
        for number in range(piece, piece + count):
            for group in range(groups):
                first = ((number - piece) * groups + group) * sub
                s.mixed[pl.ds(group * share + number * sub, sub)] = total[first : first + sub]
        for y in across:
            out_copy(y, piece, count).wait_send()
        sibling(piece, count, core).wait_send()

    def mirror(piece):
        return remote(
            s.hl_stage.at[piece],
            s.hl.at[piece],
            s.hl_send.at[piece],
            s.hl_recv.at[piece],
            "ep",
            loc + half,
        )

    def drain():
        for i in range(1, ep):
            back_copy(lax.rem(own + i, ep)).wait_send()
        for block in range(half):

            @pl.when(block != loc)
            def _():
                for piece in range(subs):
                    out_piece(block, piece).wait_send()

        for other in near:
            remote(
                query_part(other),
                s.q.at[own],
                s.q_send.at[other, 0],
                s.q_recv.at[loc, 0],
                "ep",
                side * half + other,
            ).wait_send()
        for copy in sent:
            copy.wait_send()

    @pl.when(side == 0)
    def _():
        def far_tile(piece):
            with jax.named_scope("far_wait"):
                for block in range(half):
                    target = s.q.at[half + block, pl.ds(piece * sub, sub)]
                    arrived(target, s.q_recv.at[half + block, piece])
            with jax.named_scope("far"):
                query = s.q[half:, piece * sub : (piece + 1) * sub].reshape(half * sub, size)
                carry = lax.fori_loop(
                    0, half, lambda i, c: unit(query, half - 1 - i, c, False), zeros(half * sub)
                )
            s.hl_stage[piece] = carry[0].astype(BF16)
            mirror(piece).start()

        first = jnp.where(loc < row, row, 0)
        keys_arrive(range(row))
        lax.fori_loop(0, first, local_block, 0)
        keys_arrive(range(row, half))
        ahead = max(1, subs // 2)
        for piece in range(ahead):
            far_tile(piece)
        lax.fori_loop(first, half, local_block, 0)
        for piece in range(ahead, subs):
            far_tile(piece)
        give_back()
        project(0, subs)
        combine()
        for piece in range(subs):
            mirror(piece).wait_send()
        drain()
        finish(0, subs)

    @pl.when(side == 1)
    def _():
        def merge(piece):
            with jax.named_scope("hl_wait"):
                arrived(s.hl.at[piece], s.hl_recv.at[piece])
            rows = slice(piece * sub, (piece + 1) * sub)
            s.o_stage[:, rows] = (
                s.o_part[:, rows]
                + s.passed[:, rows] * s.hl[piece].astype(F32).reshape(half, sub, size)
            ).astype(BF16)
            for block in range(half):
                hand_on(block, piece)

        keys_arrive(range(half))
        for piece in range(2, subs):
            for i in range(half):
                far_query(loc, piece, lax.rem(loc + i, half)).start()
        lax.fori_loop(0, half, local_block, 0)
        give_back()
        merge(0)
        for piece in range(1, subs):
            merge(piece)
            project(piece - 1, 1)
        project(subs - 1, 1)
        for piece in range(subs - 1):
            finish(piece, 1)
        combine()
        for piece in range(subs):
            for i in range(half):
                far_query(loc, piece, lax.rem(loc + i, half)).wait_send()
        drain()
        finish(subs - 1, 1)


def fused(p, *operands):
    dma = pltpu.SemaphoreType.DMA
    ep, tp, half, chips = p.ep, p.tp, p.half, p.chips
    per = p.slots // ep
    vmem = pl.BlockSpec(memory_space=pltpu.VMEM)
    free = pl.BlockSpec(memory_space=pl.ANY)
    small = ("bias", "gain", "ids", "scores")

    def buffer(shape, kind=BF16):
        return pltpu.VMEM(shape, kind)

    depth = p.heads * p.size
    scratch = {
        "q": buffer((ep, p.share, p.size)),
        "k": buffer((half, p.span, p.size)),
        "v": buffer((half, p.span, p.size)),
        "b": buffer((half, 8, p.span), F32),
        "b_stage": buffer((p.heads, 8, p.span), F32),
        "tri": buffer((p.width, p.width)),
        "hl_stage": buffer((p.subs, half * p.sub, p.size)),
        "hl": buffer((p.subs, half * p.sub, p.size)),
        "o_part": buffer((half, p.share, p.size), F32),
        "passed": buffer((half, p.share, p.size), F32),
        "o_stage": buffer((half, p.share, p.size)),
        "heads": buffer((2, p.span, depth)),
        "normed": buffer((p.tokens, p.features)),
        "rows_stage": buffer((ep, per, p.col)),
        "grid": buffer((p.slots, p.features)),
        "x_in": buffer((p.tokens, p.features)),
        "w_sg": buffer((p.features, p.hidden)),
        "w_su": buffer((p.features, p.hidden)),
        "w_eg": buffer((p.features, p.hidden)),
        "w_eu": buffer((p.features, p.hidden)),
        "w_sd": buffer((2, chips, p.hidden, p.col)),
        "w_ed": buffer((2, chips, p.hidden, p.col)),
        "w_o": buffer((2, chips, depth, p.col)),
        "hid": buffer((2, p.rows, p.hidden)),
        "part_send": buffer((chips, p.rows, p.col)),
        "part_recv": buffer((chips, p.rows, p.col)),
        "part_own": buffer((p.rows, p.col), F32),
        "back_stage": buffer((ep, per, p.col)),
        "back": buffer((ep, per, p.col)),
        "out_send": buffer((chips, p.span, p.col)),
        "out_recv": buffer((chips, p.span, p.col)),
        "out_own": buffer((p.span, p.col), F32),
        "load": dma((5 + 3 * chips,)),
        "kv_local": dma((4,)),
        "kv_send": dma((3, half)),
        "kv_recv": dma((3, half)),
        "q_send": dma((ep, p.subs)),
        "q_recv": dma((ep, p.subs)),
        "hl_send": dma((p.subs,)),
        "hl_recv": dma((p.subs,)),
        "o_send": dma((half, p.subs)),
        "o_recv": dma((half, p.subs)),
        "sib_send": dma((p.subs,)),
        "sib_recv": dma((p.subs,)),
        "w_send": dma((3, chips)),
        "w_recv": dma((3, chips)),
        "rows_send": dma((ep,)),
        "rows_recv": dma((ep,)),
        "relay_send": dma((ep, tp)),
        "relay_recv": dma((ep, tp)),
        "pass_send": dma((ep, tp)),
        "hid_send": dma((2,)),
        "hid_recv": dma((2,)),
        "part_ssem": dma((chips,)),
        "part_rsem": dma((chips,)),
        "back_send": dma((ep,)),
        "back_recv": dma((ep,)),
        "out_ssem": dma((chips, p.subs)),
        "out_rsem": dma((chips, p.subs)),
    }
    names = INPUTS + OUTPUTS + tuple(scratch)
    return pl.pallas_call(
        functools.partial(kernel, p, names),
        in_specs=[vmem if name in small else free for name in INPUTS],
        out_specs=[vmem, vmem],
        out_shape=[
            jax.ShapeDtypeStruct((p.span, p.col), BF16),
            jax.ShapeDtypeStruct((p.tokens, p.col), BF16),
        ],
        scratch_shapes=list(scratch.values()),
        compiler_params=pltpu.CompilerParams(
            collective_id=0, has_side_effects=True, vmem_limit_bytes=62 * 1024 * 1024
        ),
        name="fused",
    )(*operands)


def settle_kernel(mixed_in, mix_in, mixed_out, mix_out):
    mixed_out[...] = mixed_in[...]
    mix_out[...] = mix_in[...]


def settle(mixed, mix):
    vmem = pl.BlockSpec(memory_space=pltpu.VMEM)
    return pl.pallas_call(
        settle_kernel,
        in_specs=[vmem, vmem],
        out_specs=[vmem, vmem],
        out_shape=[jax.ShapeDtypeStruct(x.shape, x.dtype) for x in (mixed, mix)],
        name="settle",
    )(mixed, mix)


def body(
    queries,
    keys,
    values,
    key_bias,
    out_weight,
    moe_input,
    moe_gain,
    route_ids,
    route_scores,
    shared_gate,
    shared_up,
    shared_down,
    expert_gate,
    expert_up,
    expert_down,
):
    p = Plan(
        lax.axis_size("ep"),
        lax.axis_size("tp"),
        queries.shape,
        key_bias.shape,
        moe_input.shape,
        route_ids.shape,
        expert_gate.shape,
    )
    mixed, mix = fused(
        p,
        queries,
        keys,
        values,
        key_bias.T,
        out_weight,
        moe_input,
        moe_gain.reshape(1, -1),
        route_ids.T,
        route_scores.T,
        shared_gate,
        shared_up,
        shared_down,
        expert_gate,
        expert_up,
        expert_down,
    )
    return settle(mixed, mix)


def solution(mesh):
    return jax.shard_map(
        body,
        mesh=mesh,
        in_specs=(
            P("ep", "tp"),
            P("ep", "tp"),
            P("ep", "tp"),
            P("ep", "tp"),
            P("tp", None),
            P("ep", None),
            P(),
            P("ep", None),
            P("ep", None),
            P(None, "tp"),
            P(None, "tp"),
            P("tp", None),
            P("ep", None, "tp"),
            P("ep", None, "tp"),
            P("ep", "tp", None),
        ),
        out_specs=(P("ep", "tp"), P("ep", "tp")),
        check_vma=False,
    )
```
